32 devices in a mesh: fs: 8 (over z, y), tp: 4 (over x, core).
Axes of the slice: x: 2, y: 2, z: 4, core: 2. Of those that a mesh axis runs over, the one named last changes fastest.
Arguments:
- tokens: bfloat16 [16, 384, 2048], P('fs', None, 'tp'), may hold values from -34 to 34
- mix_gain: float32 [2048], replicated, may hold values from 0.1 to 1.9
- w_bgate: float32 [2048, 2048], P('fs', 'tp'), may hold values from -0.125 to 0.125
- w_cgate: float32 [2048, 2048], P('fs', 'tp'), may hold values from -0.125 to 0.125
- w_value: float32 [2048, 2048], P('fs', 'tp'), may hold values from -0.125 to 0.125
- in_scale: float32 [3, 2048], P(None, 'tp'), may hold values from 0.5 to 2
- mix_taps: float32 [3, 2048], P(None, 'tp'), may hold values from -3.5 to 3.5
- w_mixout: float32 [2048, 2048], P('tp', 'fs'), may hold values from -0.125 to 0.125
- mixout_scale: float32 [1, 2048], P(None, 'fs'), may hold values from 0.5 to 2
- ffn_gain: float32 [2048], replicated, may hold values from 0.1 to 1.9
- w_upgate: float32 [2048, 5632], P('fs', 'tp'), may hold values from -0.125 to 0.125
- w_upval: float32 [2048, 5632], P('fs', 'tp'), may hold values from -0.125 to 0.125
- up_scale: float32 [2, 5632], P(None, 'tp'), may hold values from 0.5 to 2
- ffn_taps: float32 [2, 3, 5632], P(None, None, 'tp'), may hold values from -3.5 to 3.5
- w_down: float32 [5632, 2048], P('tp', 'fs'), may hold values from -0.078125 to 0.078125
- down_scale: float32 [1, 2048], P(None, 'fs'), may hold values from 0.5 to 2
Outputs:
- layer_out: bfloat16 [16, 384, 2048], P('fs', None, 'tp')
The draws below stay inside these ranges and needn't reach their ends.
All inputs are finite; a program needn't handle non-finite values.
Results may differ from the reference program's by a relative error of at most 0.015.
Values may be sent and summed in bfloat16 or wider, within the bound.
A program may use at most 64 MiB of HBM per device.

```python
import math
import jax
import jax.numpy as jnp
from jax import lax

D = 2048
FF = 5632
CONV = 3
LEN = 384
SEQS = 16
N_TP = 4


def draw_tokens(key, part):
    key_base, key_rows, key_cols = jax.random.split(key, 3)
    base = jax.random.normal(key_base, (SEQS, LEN, D), jnp.float32)
    base = jnp.clip(base, -4.0, 4.0)
    row_scale = jnp.exp(jax.random.uniform(key_rows, (SEQS, LEN, 1), jnp.float32, math.log(0.3), math.log(3.0)))
    rising = jnp.exp(math.log(4.0) * (jnp.arange(D, dtype=jnp.float32) / D - 0.5))
    col_scale = rising * jax.random.uniform(key_cols, (D,), jnp.float32, 0.7, 1.4)
    return (base * row_scale * col_scale).astype(jnp.bfloat16)


def block_levels(own_key, shape, cuts, smallest, high):
    factor_of, own = 1.0, jax.random.fold_in(own_key, 6)
    for position, shards_of in cuts:
        draws = jnp.exp(jax.random.uniform(jax.random.fold_in(own, position), (shards_of,), jnp.float32, smallest / len(cuts), high / len(cuts)))
        factor_of = factor_of * jnp.repeat(draws, shape[position] // shards_of).reshape([-1 if axis == position else 1 for axis in range(len(shape))])
    return factor_of


def gaussian(rng, shape, spread, most, cuts=(), kind=jnp.bfloat16):
    loudness = block_levels(rng, shape, cuts, -0.22, 0.18) if cuts else 1.0
    drawn = jax.random.normal(rng, shape, jnp.float32) * spread * loudness
    return jnp.minimum(jnp.maximum(drawn, -most), most).astype(kind)


def setup_inputs(seed: int = 0) -> dict:
    streams_of = jax.random.split(jax.random.key(seed), 17)
    return {
        "tokens": draw_tokens(jax.random.fold_in(streams_of[16], 71), 0),
        "mix_gain": jnp.clip(1.0 + 0.18 * jax.random.normal(streams_of[1], (D,), jnp.float32), 0.1, 1.9),
        "w_bgate": gaussian(streams_of[2], (D, D), D ** -0.5, 0.125, ((0, 8), (1, 4)), jnp.float32),
        "w_cgate": gaussian(streams_of[3], (D, D), D ** -0.5, 0.125, ((0, 8), (1, 4)), jnp.float32),
        "w_value": gaussian(streams_of[4], (D, D), D ** -0.5, 0.125, ((0, 8), (1, 4)), jnp.float32),
        "in_scale": jnp.clip(jnp.exp(math.log(2.0) - 1.3862944 * jax.random.uniform(streams_of[5], (3, D), jnp.float32) ** block_levels(streams_of[5], (3, D), ((1, 4),), -0.2, 0.2)), 0.5, 2.0),
        "mix_taps": gaussian(streams_of[6], (CONV, D), CONV ** -0.5, 3.5, ((1, 4),), jnp.float32),
        "w_mixout": gaussian(streams_of[7], (D, D), D ** -0.5, 0.125, ((0, 4), (1, 8)), jnp.float32),
        "mixout_scale": jnp.clip(jnp.exp(math.log(2.0) - 1.3862944 * jax.random.uniform(streams_of[8], (1, D), jnp.float32) ** block_levels(streams_of[8], (1, D), ((1, 8),), -0.2, 0.2)), 0.5, 2.0),
        "ffn_gain": jnp.clip(1.0 + 0.18 * jax.random.normal(streams_of[9], (D,), jnp.float32), 0.1, 1.9),
        "w_upgate": gaussian(streams_of[10], (D, FF), D ** -0.5, 0.125, ((0, 8), (1, 4)), jnp.float32),
        "w_upval": gaussian(streams_of[11], (D, FF), D ** -0.5, 0.125, ((0, 8), (1, 4)), jnp.float32),
        "up_scale": jnp.clip(jnp.exp(math.log(2.0) - 1.3862944 * jax.random.uniform(streams_of[12], (2, FF), jnp.float32) ** block_levels(streams_of[12], (2, FF), ((1, 4),), -0.2, 0.2)), 0.5, 2.0),
        "ffn_taps": gaussian(streams_of[13], (2, CONV, FF), CONV ** -0.5, 3.5, ((2, 4),), jnp.float32),
        "w_down": gaussian(streams_of[14], (FF, D), FF ** -0.5, 0.078125, ((0, 4), (1, 8)), jnp.float32),
        "down_scale": jnp.clip(jnp.exp(math.log(2.0) - 1.3862944 * jax.random.uniform(streams_of[15], (1, D), jnp.float32) ** block_levels(streams_of[15], (1, D), ((1, 8),), -0.2, 0.2)), 0.5, 2.0),
    }


EPS = 1e-06

def normed_rows(values, gain):
    floats = values.astype(jnp.float32)
    factor = lax.rsqrt(lax.optimization_barrier(jnp.mean(floats * floats, axis=-1, keepdims=True)) + EPS)
    return (floats * factor * gain).astype(jnp.bfloat16).reshape(SEQS * LEN, D)

def causal_taps(values, taps):
    padded = jnp.pad(values, ((0, 0), (CONV - 1, 0), (0, 0)))
    result = jnp.zeros(values.shape, jnp.float32)
    for offset in range(CONV):
        result = result + padded[:, offset:offset + LEN] * taps[offset]
    return result

def project(inputs, matrix, scale):
    return jnp.dot(inputs, matrix.astype(jnp.bfloat16), preferred_element_type=jnp.float32) * scale

def blocked_sum(inputs, matrix, scale):
    inner_width = inputs.shape[1] // N_TP
    total = jnp.zeros((inputs.shape[0], matrix.shape[1]), jnp.float32)
    for block in range(N_TP):
        lower = block * inner_width
        part_out = jnp.dot(inputs[:, lower:lower + inner_width], matrix[lower:lower + inner_width].astype(jnp.bfloat16), preferred_element_type=jnp.float32) * scale
        rounded = lax.optimization_barrier(part_out.astype(jnp.bfloat16))
        total = total + rounded.astype(jnp.float32)
    return total

def reference(tokens, mix_gain, w_bgate, w_cgate, w_value, in_scale, mix_taps, w_mixout, mixout_scale, ffn_gain, w_upgate, w_upval, up_scale, ffn_taps, w_down, down_scale):
    row_count = SEQS * LEN
    normed = normed_rows(tokens, mix_gain)
    bgate = project(normed, w_bgate, in_scale[0])
    cgate = project(normed, w_cgate, in_scale[1])
    value = project(normed, w_value, in_scale[2])
    inner = (cgate * value).reshape(SEQS, LEN, D)
    convolved = causal_taps(inner, mix_taps)
    gated = (bgate.reshape(SEQS, LEN, D) * convolved).astype(jnp.bfloat16).reshape(row_count, D)
    mix = blocked_sum(gated, w_mixout, mixout_scale)
    resid = (tokens.reshape(row_count, D).astype(jnp.float32) + mix).astype(jnp.bfloat16)
    normed_ffn = normed_rows(resid.reshape(SEQS, LEN, D), ffn_gain)
    gate_pre = project(normed_ffn, w_upgate, up_scale[0]).reshape(SEQS, LEN, FF)
    val_pre = project(normed_ffn, w_upval, up_scale[1]).reshape(SEQS, LEN, FF)
    gate_conv = causal_taps(gate_pre, ffn_taps[0])
    val_conv = causal_taps(val_pre, ffn_taps[1])
    active = (jax.nn.silu(gate_conv) * val_conv).astype(jnp.bfloat16).reshape(row_count, FF)
    ffn = blocked_sum(active, w_down, down_scale)
    layer_out = (resid.astype(jnp.float32) + ffn).astype(jnp.bfloat16)
    return layer_out.reshape(SEQS, LEN, D)
```

```python
import functools

import jax
import jax.numpy as jnp
from jax import lax
from jax.experimental import pallas as pl
from jax.experimental.pallas import tpu as pltpu
from jax.sharding import PartitionSpec as P

EPS = 1e-06
MESH = pl.DeviceIdType.MESH
F32 = jnp.float32
BF16 = jnp.bfloat16
S, A, B, C, D = range(5)
MIX, DOWN = 0, 1


def shifted(values, by):
    rows = lax.broadcasted_iota(jnp.int32, values.shape, 0)
    return jnp.where(rows >= by, pltpu.roll(values, by, 0), 0.0)


def causal_taps(values, taps):
    return shifted(values, 2) * taps[0:1] + shifted(values, 1) * taps[1:2] + values * taps[2:3]


def join_halves(first, second, which):
    half = first.shape[-1] // 2
    lanes = lax.broadcasted_iota(jnp.int32, first.shape, 1)
    low = jnp.where(lanes < half, first, pltpu.roll(second, half, 1))
    high = jnp.where(lanes < half, pltpu.roll(first, half, 1), second)
    return jnp.where(which == 0, low, high)


def layer_kernel(
    n, n_tp, tok, gain1, gain2, iscale, mtaps, uscale, ftaps, mscale, dscale,
    w_bgate, w_cgate, w_value, w_mixout, w_upgate, w_upval, w_down, out,
    buf_s, buf_a, buf_b, buf_c, buf_d, st_a, st_b, st_c, st_d,
    f_bgate, f_cgate, f_value, f_mixout, f_upgate, f_upval, f_down,
    xg, normed, gated, active, parts, zparts, recv_core, recv_x, recv_z,
    wz_send, wz_recv, wy_send, wy_recv, ag_z_send, ag_z_recv, ag_x_send, ag_x_recv,
    ag_c_send, ag_c_recv, rs_z_send, rs_z_recv, rs_x_send, rs_x_recv, rs_c_send, rs_c_recv,
    local_sem,
):
    fs, me = lax.axis_index("fs"), lax.axis_index("tp")
    seqs, length, own = tok.shape
    width = own * n_tp
    planes, chips = n // 2, n_tp // 2
    bpo = n // n_tp
    bw = own // bpo
    sub = own // 2
    y, zz = fs % 2, fs // 2
    zi = zz % 2
    other = 1 - zi
    x, c = me // 2, me % 2
    blocks = f_upgate.shape[1] // 128
    full, odd = blocks // 2, blocks % 2
    second = full + odd
    down_rows = full * 128 + odd * 64

    def plane(r):
        result, bit = 0, 1
        while bit < planes:
            digit = zz // bit % 2
            result = result + bit * ((1 - digit) if r & bit else digit)
            bit *= 2
        return result

    def tp_of(r, core):
        return (x + r) % chips * 2 + core

    def remote(src, dst, send, recv, where):
        return pltpu.make_async_remote_copy(
            src_ref=src, dst_ref=dst, send_sem=send, recv_sem=recv,
            device_id=where, device_id_type=MESH,
        )

    bufs = (buf_s, buf_a, buf_b, buf_c, buf_d)
    stages = (None, st_a, st_b, st_c, st_d)

    def piece(g, at):
        return bufs[g].at[at, pl.ds(0, down_rows)] if g == D else bufs[g].at[at]

    def to_plane(g, r):
        src = stages[g] if r % 2 and g != S else piece(g, fs)
        return remote(
            src, piece(g, fs), wz_send.at[g, r - 1], wz_recv.at[g, r - 1],
            {"fs": plane(r) * 2 + y},
        )

    def to_row(g, r):
        at = piece(g, plane(r) * 2 + y)
        return remote(at, at, wy_send.at[g, r], wy_recv.at[g, r], {"fs": fs + 1 - 2 * y})

    def launch(g, rs):
        for r in rs:
            if r:
                to_plane(g, r).start()
            else:
                to_row(g, 0).start()

    def arrive(g, rs):
        for r in rs:
            to_plane(g, r).wait_recv()
            to_row(g, r).start()

    def complete(g):
        for r in range(planes):
            to_row(g, r).wait_recv()

    across = range(1, planes)

    def ag_z(k, s, src=None):
        at = xg.at[zi, me, s]
        return remote(
            at if src is None else src, at, ag_z_send.at[k, s], ag_z_recv.at[k, s],
            {"fs": fs + 2 - 4 * zi},
        )

    def ag_x(k, s, r, i, src=None):
        at = xg.at[other if i else zi, me, s]
        return remote(
            at if src is None else src, at, ag_x_send.at[k, s, r - 1, i],
            ag_x_recv.at[k, s, r - 1, i], {"tp": tp_of(r, c)},
        )

    def ag_c(k, s, r, i, src=None):
        at = xg.at[other if i else zi, tp_of(chips - r, c), s]
        return remote(
            at if src is None else src, at, ag_c_send.at[k, s, r, i], ag_c_recv.at[k, s, r, i],
            {"tp": me + 1 - 2 * c},
        )

    def gather_own(k, s, src=None):
        ag_z(k, s, src).start()
        for r in range(1, chips):
            ag_x(k, s, r, 0, src).start()
        ag_c(k, s, 0, 0, src).start()

    def gather_z(k, s):
        ag_z(k, s).wait_recv()
        for r in range(1, chips):
            ag_x(k, s, r, 1).start()
        ag_c(k, s, 0, 1).start()

    def gather_x(k, s):
        for i in (0, 1):
            for r in range(1, chips):
                ag_x(k, s, r, i).wait_recv()
                ag_c(k, s, r, i).start()

    def gather_done(k, s):
        for i in (0, 1):
            for r in range(chips):
                ag_c(k, s, r, i).wait_recv()

    def gather_sent(k, src=None):
        for s in range(seqs):
            ag_z(k, s).wait_send()
            for i in (0, 1):
                for r in range(1, chips):
                    ag_x(k, s, r, i).wait_send()
                for r in range(chips):
                    ag_c(k, s, r, i).wait_send()

    def rs_c(k, s, r):
        return remote(
            parts.at[r, 1, s], recv_core.at[k, r, s], rs_c_send.at[k, s, r],
            rs_c_recv.at[k, s, r], {"tp": me + 1 - 2 * c},
        )

    def rs_x(k, s, r):
        return remote(
            parts.at[r, 0, s], recv_x.at[k, r - 1, s], rs_x_send.at[k, s, r - 1],
            rs_x_recv.at[k, s, r - 1], {"tp": tp_of(r, c)},
        )

    def rs_z(k, s):
        return remote(
            zparts.at[s], recv_z.at[k, s], rs_z_send.at[k, s], rs_z_recv.at[k, s],
            {"fs": fs + 2 - 4 * zi},
        )

    def products(k, s, r, side):
        owner = tp_of(r, 1 - c if side else c)
        source, held = ((gated, buf_b), (active, buf_d))[k]
        for i in (0, 1):
            for b in range(bpo):
                at = owner * bpo + b
                part = jnp.dot(source[s, i], held[at], preferred_element_type=F32)
                parts[r, side, s, i, :, b * bw : (b + 1) * bw] = (
                    part * buf_s[at, k : k + 1, :]
                ).astype(BF16)

    order = list(range(1, chips)) + [0]
    tile = 64

    def scatter_begin(k, s):
        for r in order:
            products(k, s, r, 1)
            rs_c(k, s, r).start()
        for r in order:
            products(k, s, r, 0)

    def scatter_x(k, s):
        for r in range(1, chips):
            rs_c(k, s, r).wait_recv()

            def step(j, carry, r=r):
                at = pl.ds(pl.multiple_of(j * tile, tile), tile)
                for i in (0, 1):
                    total = parts[r, 0, s, i, at, :].astype(F32)
                    total = total + recv_core[k, r, s, i, at, :].astype(F32)
                    parts[r, 0, s, i, at, :] = total.astype(BF16)
                return carry

            lax.fori_loop(0, length // tile, step, 0)
            rs_x(k, s, r).start()

    def quad(k, s, i, at):
        total = parts[0, 0, s, i, at, :].astype(F32) + recv_core[k, 0, s, i, at, :].astype(F32)
        for r in range(1, chips):
            total = total + recv_x[k, r - 1, s, i, at, :].astype(F32)
        return total

    def scatter_z(k, s):
        rs_c(k, s, 0).wait_recv()
        for r in range(1, chips):
            rs_x(k, s, r).wait_recv()

        def step(j, carry):
            at = pl.ds(pl.multiple_of(j * tile, tile), tile)
            zparts[s, at, :] = quad(k, s, other, at).astype(BF16)
            return carry

        lax.fori_loop(0, length // tile, step, 0)
        rs_z(k, s).start()

    def scatter_end(k, s, base, store):
        rs_z(k, s).wait_recv()

        def step(j, carry):
            at = pl.ds(pl.multiple_of(j * tile, tile), tile)
            total = quad(k, s, zi, at) + recv_z[k, s, at, :].astype(F32)
            store(at, (base(at).astype(F32) + total).astype(BF16))
            return carry

        lax.fori_loop(0, length // tile, step, 0)

    def scatter_sent(k):
        for s in range(seqs):
            for r in range(chips):
                rs_c(k, s, r).wait_send()
                if r:
                    rs_x(k, s, r).wait_send()
            rs_z(k, s).wait_send()

    barrier = pltpu.get_barrier_semaphore()
    peers = [{"fs": plane(r) * 2 + y} for r in across]
    peers += [{"fs": fs + 1 - 2 * y}, {"tp": me + 1 - 2 * c}]
    peers += [{"tp": tp_of(r, c)} for r in range(1, chips)]
    for peer in peers:
        pl.semaphore_signal(barrier, inc=1, device_id=peer, device_id_type=MESH)

    sources = (w_bgate, w_cgate, w_value, w_mixout, w_upgate, w_upval, w_down)
    floats = (f_bgate, f_cgate, f_value, f_mixout, f_upgate, f_upval, f_down)
    loads = [
        pltpu.make_async_copy(source, held, local_sem.at[i])
        for i, (source, held) in enumerate(zip(sources, floats))
    ]
    for copy in loads:
        copy.start()

    def cast_rows(rows, put):
        step_rows = 32

        def step(i, carry):
            put(i * step_rows, step_rows)
            return carry

        lax.fori_loop(0, rows // step_rows, step, 0)

    def rows_at(start, count):
        return pl.ds(pl.multiple_of(start, 32), count)

    def lanes_at(start, count):
        return pl.ds(pl.multiple_of(start, 128), count)

    def put_in(start, count):
        at = rows_at(start, count)
        for i, held in enumerate((f_bgate, f_cgate, f_value)):
            cols = slice(i * sub, (i + 1) * sub)
            buf_a[fs, at, cols] = held[at, lanes_at(zi * sub, sub)].astype(BF16)
            st_a[at, cols] = held[at, lanes_at(other * sub, sub)].astype(BF16)

    def put_mixout(start, count):
        at = rows_at(start, count)
        buf_b[fs, at, :] = f_mixout[rows_at(zi * sub + start, count), :].astype(BF16)
        st_b[at, :] = f_mixout[rows_at(other * sub + start, count), :].astype(BF16)

    def put_up(start, count):
        at = rows_at(start, count)
        for j in range(full):
            for i, held in enumerate((f_upgate, f_upval)):
                cols = slice(j * 256 + i * 128, j * 256 + i * 128 + 128)
                mine = lanes_at((zi * second + j) * 128, 128)
                theirs = lanes_at((other * second + j) * 128, 128)
                buf_c[fs, at, cols] = held[at, mine].astype(BF16)
                st_c[at, cols] = held[at, theirs].astype(BF16)
        if odd:
            mid = slice(full * 128, full * 128 + 128)
            cols = slice(full * 256, full * 256 + 128)
            gate, val = f_upgate[at, mid], f_upval[at, mid]
            buf_c[fs, at, cols] = join_halves(gate, val, zi).astype(BF16)
            st_c[at, cols] = join_halves(gate, val, other).astype(BF16)

    def put_down(start, count):
        at = rows_at(start, count)
        buf_d[fs, at, :] = f_down[rows_at(zi * second * 128 + start, count), :].astype(BF16)
        st_d[at, :] = f_down[rows_at(other * second * 128 + start, count), :].astype(BF16)

    def put_down_mid(start, count):
        base = full * 128
        at = rows_at(base + start, count)
        buf_d[fs, at, :] = f_down[rows_at(base + zi * 64 + start, count), :].astype(BF16)
        st_d[at, :] = f_down[rows_at(base + other * 64 + start, count), :].astype(BF16)

    buf_s[fs] = jnp.zeros(buf_s.shape[1:], F32)
    buf_s[fs, 0:1, :] = mscale[...]
    buf_s[fs, 1:2, :] = dscale[...]
    for i in range(3):
        loads[i].wait()
    cast_rows(f_bgate.shape[0], put_in)
    pl.semaphore_wait(barrier, len(peers))

    launch(S, range(planes))
    gather_own(MIX, 0, tok.at[0])
    launch(A, [0] + list(across))
    for s in range(1, seqs):
        gather_own(MIX, s, tok.at[s])
    xg[zi, me] = tok[...]
    loads[3].wait()
    cast_rows(sub, put_mixout)
    launch(B, [0] + list(across))
    for i in (4, 5, 6):
        loads[i].wait()
    cast_rows(f_upgate.shape[0], put_up)
    cast_rows(full * 128, put_down)
    if odd:
        cast_rows(64, put_down_mid)
        for at in range(n):
            buf_d[at, down_rows:, :] = jnp.zeros((64, bw), BF16)

    def normalize(s, gain):
        step_rows = 32

        def step(j, carry):
            at = pl.ds(pl.multiple_of(j * step_rows, step_rows), step_rows)
            for i in (0, 1):
                squares = jnp.zeros((step_rows, 1), F32)
                for t in range(n_tp):
                    values = xg[i, t, s, at, :].astype(F32)
                    squares = squares + jnp.sum(values * values, axis=-1, keepdims=True)
                factor = lax.rsqrt(squares * (1.0 / width) + EPS)
                for t in range(n_tp):
                    cols = slice(t * own, (t + 1) * own)
                    values = xg[i, t, s, at, :].astype(F32)
                    normed[s, i, at, cols] = (values * factor * gain[:, cols]).astype(BF16)
            return carry

        lax.fori_loop(0, length // step_rows, step, 0)

    arrive(S, across)
    gather_z(MIX, 0)
    arrive(A, [1])
    for s in range(1, seqs):
        gather_z(MIX, s)
    gather_x(MIX, 0)
    for r in across:
        if r > 1:
            arrive(A, [r])
    for s in range(1, seqs):
        gather_x(MIX, s)
    launch(C, [0, 1])
    arrive(B, across)
    for s in range(seqs):
        gather_done(MIX, s)
        normalize(s, gain1)
    complete(S)
    complete(A)

    mixed = min(256, sub)

    def mixer(s):
        def step(j, carry):
            i, at = j % 2, j // 2 * mixed

            def product(m):
                cols = pl.ds(pl.multiple_of(m * sub + at, 128), mixed)
                matrix = buf_a[:, :, cols].reshape(width, mixed)
                return jnp.dot(normed[s, i], matrix, preferred_element_type=F32)

            here = pl.ds(pl.multiple_of(zi * sub + at, 128), mixed)
            scales = iscale[:, here]
            inner = (product(1) * scales[1:2]) * (product(2) * scales[2:3])
            convolved = causal_taps(inner, mtaps[:, here])
            cols = pl.ds(pl.multiple_of(at, 128), mixed)
            gated[s, i, :, cols] = (product(0) * scales[0:1] * convolved).astype(BF16)
            return carry

        lax.fori_loop(0, 2 * (sub // mixed), step, 0)

    mixer(0)
    if planes > 2:
        launch(C, [2])
    for s in range(1, seqs):
        mixer(s)
    gather_sent(MIX)
    complete(B)
    for s in range(seqs):
        scatter_begin(MIX, s)
        scatter_x(MIX, s)
    arrive(C, [1])
    launch(C, range(3, planes))
    launch(D, [0])

    for s in range(seqs):
        scatter_z(MIX, s)
    for s in range(seqs):

        def store_resid(at, values, s=s):
            xg[zi, me, s, at, :] = values

        scatter_end(MIX, s, lambda at, s=s: tok[s, at, :], store_resid)
        gather_own(DOWN, s)
    for s in range(seqs):
        gather_z(DOWN, s)
    launch(D, across)
    for s in range(seqs):
        gather_x(DOWN, s)
    for r in across:
        if r > 1:
            arrive(C, [r])
    for s in range(seqs):
        gather_done(DOWN, s)
        normalize(s, gain2)
    complete(C)

    def up(s):
        def activate(gate, val):
            return gate / (1.0 + jnp.exp(-gate)) * val

        def step(j, carry):
            i, t = j % 2, j // 2
            matrix = buf_c[:, :, lanes_at(t * 256, 256)].reshape(width, 256)
            both = jnp.dot(normed[s, i], matrix, preferred_element_type=F32)
            here = lanes_at((zi * second + t) * 128, 128)
            gate = causal_taps(both[:, :128] * uscale[0:1, here], ftaps[0, :, here])
            val = causal_taps(both[:, 128:] * uscale[1:2, here], ftaps[1, :, here])
            active[s, i, :, lanes_at(t * 128, 128)] = activate(gate, val).astype(BF16)
            return carry

        lax.fori_loop(0, 2 * full, step, 0)
        if odd:
            mid = slice(full * 128, full * 128 + 128)
            scale = join_halves(uscale[0:1, mid], uscale[1:2, mid], zi)
            taps = join_halves(ftaps[0, :, mid], ftaps[1, :, mid], zi)

            def last(i, carry):
                matrix = buf_c[:, :, full * 256 :].reshape(width, 128)
                both = jnp.dot(normed[s, i], matrix, preferred_element_type=F32)
                gate = causal_taps(both * scale, taps)
                values = activate(gate, pltpu.roll(gate, 64, 1))
                lanes = lax.broadcasted_iota(jnp.int32, values.shape, 1)
                active[s, i, :, mid] = jnp.where(lanes < 64, values, 0.0).astype(BF16)
                return carry

            lax.fori_loop(0, 2, last, 0)

    for s in range(seqs):
        up(s)
        if s == 0:
            arrive(D, across)
    scatter_sent(MIX)
    complete(D)

    for s in range(seqs):
        scatter_begin(DOWN, s)
        scatter_x(DOWN, s)
    for s in range(seqs):
        scatter_z(DOWN, s)
    for s in range(seqs):

        def store_out(at, values, s=s):
            out[s, at, :] = values

        scatter_end(DOWN, s, lambda at, s=s: xg[zi, me, s, at, :], store_out)

    gather_sent(DOWN)
    scatter_sent(DOWN)
    for g in range(5):
        for r in range(planes):
            to_row(g, r).wait_send()
            if r:
                to_plane(g, r).wait_send()


def on_device(
    n,
    n_tp,
    tokens,
    mix_gain,
    w_bgate,
    w_cgate,
    w_value,
    in_scale,
    mix_taps,
    w_mixout,
    mixout_scale,
    ffn_gain,
    w_upgate,
    w_upval,
    up_scale,
    ffn_taps,
    w_down,
    down_scale,
):
    seqs, length, own = tokens.shape
    width = own * n_tp
    part = w_bgate.shape[0]
    ff = w_upgate.shape[1]
    pad = -ff % 128
    ffp = ff + pad
    bw = w_mixout.shape[1]

    if pad:
        w_upgate, w_upval, up_scale, ffn_taps = (
            jnp.pad(x, [(0, 0)] * (x.ndim - 1) + [(0, pad)])
            for x in (w_upgate, w_upval, up_scale, ffn_taps)
        )
        w_down = jnp.pad(w_down, ((0, pad), (0, 0)))
    weights = (w_bgate, w_cgate, w_value, w_mixout, w_upgate, w_upval, w_down)
    planes, chips, sub = n // 2, n_tp // 2, own // 2
    full, odd = ffp // 128 // 2, ffp // 128 % 2
    hidden, down_rows = (full + odd) * 128, full * 128 + odd * 64
    vmem, dma = pltpu.VMEM, pltpu.SemaphoreType.DMA
    result = pl.pallas_call(
        functools.partial(layer_kernel, n, n_tp),
        out_shape=jax.ShapeDtypeStruct((seqs, length, own), BF16),
        in_specs=[pl.BlockSpec(memory_space=pltpu.VMEM)] * 9
        + [pl.BlockSpec(memory_space=pl.ANY)] * 7,
        out_specs=pl.BlockSpec(memory_space=pltpu.VMEM),
        scratch_shapes=[
            vmem((n, 8, bw), F32),
            vmem((n, part, 3 * sub), BF16),
            vmem((n, sub, bw), BF16),
            vmem((n, part, ffp), BF16),
            vmem((n, hidden, bw), BF16),
            vmem((part, 3 * sub), BF16),
            vmem((sub, bw), BF16),
            vmem((part, ffp), BF16),
            vmem((down_rows, bw), BF16),
        ]
        + [vmem(w.shape, F32) for w in weights]
        + [
            vmem((2, n_tp, seqs, length, own), BF16),
            vmem((seqs, 2, length, width), BF16),
            vmem((seqs, 2, length, sub), BF16),
            vmem((seqs, 2, length, hidden), BF16),
            vmem((chips, 2, seqs, 2, length, own), BF16),
            vmem((seqs, length, own), BF16),
            vmem((2, chips, seqs, 2, length, own), BF16),
            vmem((2, chips - 1, seqs, 2, length, own), BF16),
            vmem((2, seqs, length, own), BF16),
            dma((5, planes - 1)),
            dma((5, planes - 1)),
            dma((5, planes)),
            dma((5, planes)),
            dma((2, seqs)),
            dma((2, seqs)),
            dma((2, seqs, chips - 1, 2)),
            dma((2, seqs, chips - 1, 2)),
            dma((2, seqs, chips, 2)),
            dma((2, seqs, chips, 2)),
            dma((2, seqs)),
            dma((2, seqs)),
            dma((2, seqs, chips - 1)),
            dma((2, seqs, chips - 1)),
            dma((2, seqs, chips)),
            dma((2, seqs, chips)),
            dma((7,)),
        ],
        compiler_params=pltpu.CompilerParams(
            collective_id=0, has_side_effects=True, vmem_limit_bytes=67043328
        ),
        name="layer",
    )(
        tokens, mix_gain.reshape(1, width), ffn_gain.reshape(1, width),
        in_scale, mix_taps, up_scale, ffn_taps, mixout_scale, down_scale, *weights,
    )
    return result


def solution(mesh):
    in_specs = (
        P("fs", None, "tp"),
        P(),
        P("fs", "tp"),
        P("fs", "tp"),
        P("fs", "tp"),
        P(None, "tp"),
        P(None, "tp"),
        P("tp", "fs"),
        P(None, "fs"),
        P(),
        P("fs", "tp"),
        P("fs", "tp"),
        P(None, "tp"),
        P(None, None, "tp"),
        P("tp", "fs"),
        P(None, "fs"),
    )
    out_specs = P("fs", None, "tp")
    body = functools.partial(on_device, mesh.shape["fs"], mesh.shape["tp"])
    return jax.shard_map(body, mesh=mesh, in_specs=in_specs, out_specs=out_specs, check_vma=False)
```

```python
import functools

import jax
import jax.numpy as jnp
from jax import lax
from jax.experimental import pallas as pl
from jax.experimental.pallas import tpu as pltpu
from jax.sharding import PartitionSpec as P

EPS = 1e-06
MESH = pl.DeviceIdType.MESH
F32 = jnp.float32
BF16 = jnp.bfloat16
S, A, F, B, C, E, D, G = range(8)
MIX, DOWN = 0, 1


def shifted(values, by):
    rows = lax.broadcasted_iota(jnp.int32, values.shape, 0)
    return jnp.where(rows >= by, pltpu.roll(values, by, 0), 0.0)


def causal_taps(values, taps):
    return shifted(values, 2) * taps[0:1] + shifted(values, 1) * taps[1:2] + values * taps[2:3]


def join_halves(first, second, which):
    half = first.shape[-1] // 2
    lanes = lax.broadcasted_iota(jnp.int32, first.shape, 1)
    low = jnp.where(lanes < half, first, pltpu.roll(second, half, 1))
    high = jnp.where(lanes < half, pltpu.roll(first, half, 1), second)
    return jnp.where(which == 0, low, high)


def layer_kernel(
    n, n_tp, tok, gain1, gain2, iscale, mtaps, uscale, ftaps, mscale, dscale,
    w_bgate, w_cgate, w_value, w_mixout, w_upgate, w_upval, w_down, out,
    buf_s, buf_a, buf_b, buf_c, buf_d, st_a, st_b, st_c, st_d,
    f_bgate, f_cgate, f_value, f_mixout, f_upgate, f_upval, f_down,
    xg, normed, gated, active, parts, zparts, recv_core, recv_x, recv_z,
    wz_send, wz_recv, wy_send, wy_recv, ag_z_send, ag_z_recv, ag_x_send, ag_x_recv,
    ag_c_send, ag_c_recv, rs_z_send, rs_z_recv, rs_x_send, rs_x_recv, rs_c_send, rs_c_recv,
    local_sem,
):
    fs, me = lax.axis_index("fs"), lax.axis_index("tp")
    seqs, length, own = tok.shape
    width = own * n_tp
    planes, chips = n // 2, n_tp // 2
    bpo = n // n_tp
    bw = own // bpo
    sub = own // 2
    y, zz = fs % 2, fs // 2
    zi = zz % 2
    other = 1 - zi
    x, c = me // 2, me % 2
    blocks = f_upgate.shape[1] // 128
    full, odd = blocks // 2, blocks % 2
    second = full + odd
    down_rows = full * 128 + odd * 64

    def plane(r):
        result, bit = 0, 1
        while bit < planes:
            digit = zz // bit % 2
            result = result + bit * ((1 - digit) if r & bit else digit)
            bit *= 2
        return result

    def tp_of(r, core):
        return (x + r) % chips * 2 + core

    def remote(src, dst, send, recv, where):
        return pltpu.make_async_remote_copy(
            src_ref=src, dst_ref=dst, send_sem=send, recv_sem=recv,
            device_id=where, device_id_type=MESH,
        )

    bufs = (buf_s, buf_a, buf_a, buf_b, buf_c, buf_c, buf_d, buf_d)
    stages = (None, st_a, st_a, st_b, st_c, st_c, st_d, st_d)
    half = buf_c.shape[1] // 2
    low, high = pl.ds(0, half), pl.ds(half, half)
    spans = {A: low, F: high, C: low, E: high}
    spans[D] = pl.ds(0, down_rows // 2)
    spans[G] = pl.ds(down_rows // 2, down_rows // 2)

    def piece(g, at):
        return bufs[g].at[at, spans[g]] if g in spans else bufs[g].at[at]

    def stage(g):
        return stages[g].at[spans[g]] if g in spans else stages[g]

    def to_plane(g, r):
        src = stage(g) if r % 2 and g != S else piece(g, fs)
        return remote(
            src, piece(g, fs), wz_send.at[g, r - 1], wz_recv.at[g, r - 1],
            {"fs": plane(r) * 2 + y},
        )

    def to_row(g, r):
        at = piece(g, plane(r) * 2 + y)
        return remote(at, at, wy_send.at[g, r], wy_recv.at[g, r], {"fs": fs + 1 - 2 * y})

    def launch(g, rs):
        for r in rs:
            if r:
                to_plane(g, r).start()
            else:
                to_row(g, 0).start()

    def arrive(g, rs):
        for r in rs:
            to_plane(g, r).wait_recv()
            to_row(g, r).start()

    def complete(g):
        for r in range(planes):
            to_row(g, r).wait_recv()

    across = range(1, planes)
    rest = list(across)[:0:-1]

    def ag_z(k, s, src=None):
        at = xg.at[zi, me, s]
        return remote(
            at if src is None else src, at, ag_z_send.at[k, s], ag_z_recv.at[k, s],
            {"fs": fs + 2 - 4 * zi},
        )

    def ag_x(k, s, r, i, src=None):
        at = xg.at[other if i else zi, me, s]
        return remote(
            at if src is None else src, at, ag_x_send.at[k, s, r - 1, i],
            ag_x_recv.at[k, s, r - 1, i], {"tp": tp_of(r, c)},
        )

    def ag_c(k, s, r, i, src=None):
        at = xg.at[other if i else zi, tp_of(chips - r, c), s]
        return remote(
            at if src is None else src, at, ag_c_send.at[k, s, r, i], ag_c_recv.at[k, s, r, i],
            {"tp": me + 1 - 2 * c},
        )

    def gather_own(k, s, src=None):
        ag_z(k, s, src).start()
        for r in range(1, chips):
            ag_x(k, s, r, 0, src).start()
        ag_c(k, s, 0, 0, src).start()

    def gather_z(k, s):
        ag_z(k, s).wait_recv()
        for r in range(1, chips):
            ag_x(k, s, r, 1).start()
        ag_c(k, s, 0, 1).start()

    def gather_x(k, s):
        for i in (0, 1):
            for r in range(1, chips):
                ag_x(k, s, r, i).wait_recv()
                ag_c(k, s, r, i).start()

    def gather_done(k, s):
        for i in (0, 1):
            for r in range(chips):
                ag_c(k, s, r, i).wait_recv()

    def gather_sent(k):
        for s in range(seqs):
            if k == MIX:
                ag_z(k, s).wait_send()
            for i in (0, 1):
                for r in range(1, chips):
                    ag_x(k, s, r, i).wait_send()
                for r in range(chips):
                    ag_c(k, s, r, i).wait_send()

    def rs_c(k, s, r):
        return remote(
            parts.at[r, 1, s], recv_core.at[k, r, s], rs_c_send.at[k, s, r],
            rs_c_recv.at[k, s, r], {"tp": me + 1 - 2 * c},
        )

    def rs_x(k, s, r):
        return remote(
            parts.at[r, 0, s], recv_x.at[k, r - 1, s], rs_x_send.at[k, s, r - 1],
            rs_x_recv.at[k, s, r - 1], {"tp": tp_of(r, c)},
        )

    def rs_z(k, s):
        src, dst = zparts.at[s], recv_z.at[k, s]
        if k == DOWN:
            src, dst = zparts.at[s, other], recv_z.at[k, s, 0]
        return remote(
            src, dst, rs_z_send.at[k, s], rs_z_recv.at[k, s], {"fs": fs + 2 - 4 * zi},
        )

    def products(k, s, r, side):
        owner = tp_of(r, 1 - c if side else c)
        source, held = ((gated, buf_b), (active, buf_d))[k]
        for i in (0, 1):
            for b in range(bpo):
                at = owner * bpo + b
                part = jnp.dot(source[s, i], held[at], preferred_element_type=F32)
                parts[r, side, s, i, :, b * bw : (b + 1) * bw] = (
                    part * buf_s[at, k : k + 1, :]
                ).astype(BF16)

    order = list(range(1, chips)) + [0]
    tile = 64

    def scatter_begin(k, s, rs):
        for r in rs:
            products(k, s, r, 1)
            rs_c(k, s, r).start()
        for r in rs:
            products(k, s, r, 0)

    def away(r):
        return plane(r) // 2 != x

    def each_down(test, do):
        for r in [0, 1] + rest:

            @pl.when(test(r))
            def _(r=r):
                for g in (D, G):
                    do(g, r)

    def down_launch(first):
        @pl.when(away(0) == first)
        def _():
            for r in [0, 1] + rest:
                launch(D, [r])
                launch(G, [r])

    def down_arrive(first):
        def do(g, r):
            if r:
                arrive(g, [r])

        each_down(lambda r: away(r) == first, do)

    def down_complete(first):
        each_down(lambda r: away(r) == first, lambda g, r: to_row(g, r).wait_recv())

    def scatter_x(k, s):
        for r in range(1, chips):
            rs_c(k, s, r).wait_recv()

            def step(j, carry, r=r):
                at = pl.ds(pl.multiple_of(j * tile, tile), tile)
                for i in (0, 1):
                    total = parts[r, 0, s, i, at, :].astype(F32)
                    total = total + recv_core[k, r, s, i, at, :].astype(F32)
                    parts[r, 0, s, i, at, :] = total.astype(BF16)
                return carry

            lax.fori_loop(0, length // tile, step, 0)
            rs_x(k, s, r).start()

    def quad(k, s, i, at):
        total = parts[0, 0, s, i, at, :].astype(F32) + recv_core[k, 0, s, i, at, :].astype(F32)
        for r in range(1, chips):
            total = total + recv_x[k, r - 1, s, i, at, :].astype(F32)
        return total

    def scatter_z(k, s):
        rs_c(k, s, 0).wait_recv()
        for r in range(1, chips):
            rs_x(k, s, r).wait_recv()

        def step(j, carry):
            at = pl.ds(pl.multiple_of(j * tile, tile), tile)
            for i in (0, 1) if k == MIX else (other,):
                zparts[s, i, at, :] = quad(k, s, i, at).astype(BF16)
            return carry

        lax.fori_loop(0, length // tile, step, 0)
        rs_z(k, s).start()

    def resid(s):
        rs_z(MIX, s).wait_recv()

        def step(j, carry):
            at = pl.ds(pl.multiple_of(j * tile, tile), tile)
            for i in (0, 1):
                total = zparts[s, i, at, :].astype(F32) + recv_z[MIX, s, i, at, :].astype(F32)
                xg[i, me, s, at, :] = (xg[i, me, s, at, :].astype(F32) + total).astype(BF16)
            return carry

        lax.fori_loop(0, length // tile, step, 0)
        for i in (0, 1):
            for r in range(1, chips):
                ag_x(DOWN, s, r, i).start()
            ag_c(DOWN, s, 0, i).start()

    def finish(s):
        rs_z(DOWN, s).wait_recv()

        def step(j, carry):
            at = pl.ds(pl.multiple_of(j * tile, tile), tile)
            total = quad(DOWN, s, zi, at) + recv_z[DOWN, s, 0, at, :].astype(F32)
            out[s, at, :] = (xg[zi, me, s, at, :].astype(F32) + total).astype(BF16)
            return carry

        lax.fori_loop(0, length // tile, step, 0)

    def scatter_sent(k):
        for s in range(seqs):
            for r in range(chips):
                rs_c(k, s, r).wait_send()
                if r:
                    rs_x(k, s, r).wait_send()
            rs_z(k, s).wait_send()

    barrier = pltpu.get_barrier_semaphore()
    peers = [{"fs": plane(r) * 2 + y} for r in across]
    peers += [{"fs": fs + 1 - 2 * y}, {"tp": me + 1 - 2 * c}]
    peers += [{"tp": tp_of(r, c)} for r in range(1, chips)]
    for peer in peers:
        pl.semaphore_signal(barrier, inc=1, device_id=peer, device_id_type=MESH)

    sources = (w_bgate, w_cgate, w_value, w_mixout, w_upgate, w_upval, w_down)
    floats = (f_bgate, f_cgate, f_value, f_mixout, f_upgate, f_upval, f_down)
    loads = [
        pltpu.make_async_copy(source, held, local_sem.at[i])
        for i, (source, held) in enumerate(zip(sources, floats))
    ]
    for copy in loads:
        copy.start()

    def cast_rows(rows, put):
        step_rows = 32

        def step(i, carry):
            put(i * step_rows, step_rows)
            return carry

        lax.fori_loop(0, rows // step_rows, step, 0)

    def rows_at(start, count):
        return pl.ds(pl.multiple_of(start, 32), count)

    def lanes_at(start, count):
        return pl.ds(pl.multiple_of(start, 128), count)

    def put_in(start, count):
        at = rows_at(start, count)
        for i, held in enumerate((f_bgate, f_cgate, f_value)):
            cols = slice(i * sub, (i + 1) * sub)
            buf_a[fs, at, cols] = held[at, lanes_at(zi * sub, sub)].astype(BF16)
            st_a[at, cols] = held[at, lanes_at(other * sub, sub)].astype(BF16)

    def put_mixout(start, count):
        at = rows_at(start, count)
        buf_b[fs, at, :] = f_mixout[rows_at(zi * sub + start, count), :].astype(BF16)
        st_b[at, :] = f_mixout[rows_at(other * sub + start, count), :].astype(BF16)

    def put_up(start, count):
        at = rows_at(start, count)
        for j in range(full):
            for i, held in enumerate((f_upgate, f_upval)):
                cols = slice(j * 256 + i * 128, j * 256 + i * 128 + 128)
                mine = lanes_at((zi * second + j) * 128, 128)
                theirs = lanes_at((other * second + j) * 128, 128)
                buf_c[fs, at, cols] = held[at, mine].astype(BF16)
                st_c[at, cols] = held[at, theirs].astype(BF16)
        if odd:
            mid = slice(full * 128, full * 128 + 128)
            cols = slice(full * 256, full * 256 + 128)
            gate, val = f_upgate[at, mid], f_upval[at, mid]
            buf_c[fs, at, cols] = join_halves(gate, val, zi).astype(BF16)
            st_c[at, cols] = join_halves(gate, val, other).astype(BF16)

    def put_down(start, count):
        at = rows_at(start, count)
        buf_d[fs, at, :] = f_down[rows_at(zi * second * 128 + start, count), :].astype(BF16)
        st_d[at, :] = f_down[rows_at(other * second * 128 + start, count), :].astype(BF16)

    def put_down_mid(start, count):
        base = full * 128
        at = rows_at(base + start, count)
        buf_d[fs, at, :] = f_down[rows_at(base + zi * 64 + start, count), :].astype(BF16)
        st_d[at, :] = f_down[rows_at(base + other * 64 + start, count), :].astype(BF16)

    buf_s[fs] = jnp.zeros(buf_s.shape[1:], F32)
    buf_s[fs, 0:1, :] = mscale[...]
    buf_s[fs, 1:2, :] = dscale[...]
    for i in range(3):
        loads[i].wait()
    cast_rows(f_bgate.shape[0], put_in)
    pl.semaphore_wait(barrier, len(peers))

    launch(S, range(planes))
    gather_own(MIX, 0, tok.at[0])
    for g in (A, F):
        launch(g, [0, 1])
    for s in range(1, seqs):
        gather_own(MIX, s, tok.at[s])
    for r in rest:
        launch(A, [r])
        launch(F, [r])
    xg[zi, me] = tok[...]
    loads[3].wait()
    cast_rows(sub, put_mixout)
    launch(B, [0, 1])
    launch(B, rest)
    for i in (4, 5, 6):
        loads[i].wait()
    cast_rows(f_upgate.shape[0], put_up)
    cast_rows(full * 128, put_down)
    if odd:
        cast_rows(64, put_down_mid)
        for at in range(n):
            buf_d[at, down_rows:, :] = jnp.zeros((64, bw), BF16)

    def normalize(s, gain):
        step_rows = 32

        def step(j, carry):
            at = pl.ds(pl.multiple_of(j * step_rows, step_rows), step_rows)
            for i in (0, 1):
                squares = jnp.zeros((step_rows, 1), F32)
                for t in range(n_tp):
                    values = xg[i, t, s, at, :].astype(F32)
                    squares = squares + jnp.sum(values * values, axis=-1, keepdims=True)
                factor = lax.rsqrt(squares * (1.0 / width) + EPS)
                for t in range(n_tp):
                    cols = slice(t * own, (t + 1) * own)
                    values = xg[i, t, s, at, :].astype(F32)
                    normed[s, i, at, cols] = (values * factor * gain[:, cols]).astype(BF16)
            return carry

        lax.fori_loop(0, length // step_rows, step, 0)

    arrive(S, across)
    gather_z(MIX, 0)
    arrive(A, rest[:1])
    arrive(A, [1])
    gather_x(MIX, 0)
    arrive(F, rest[:1])
    arrive(F, [1])
    arrive(A, rest[1:])
    arrive(F, rest[1:])
    for s in range(1, seqs):
        gather_z(MIX, s)
    gather_done(MIX, 0)
    normalize(0, gain1)
    launch(C, [1])
    arrive(B, across)
    for s in range(1, seqs):
        gather_x(MIX, s)
        gather_done(MIX, s)
        normalize(s, gain1)
    launch(E, [1])
    for r in rest:
        launch(C, [r])
        launch(E, [r])
    launch(C, [0])
    complete(S)
    complete(A)
    complete(F)

    mixed = min(256, sub)

    def mixer(s):
        def step(j, carry):
            i, at = j % 2, j // 2 * mixed

            def product(m):
                cols = pl.ds(pl.multiple_of(m * sub + at, 128), mixed)
                matrix = buf_a[:, :, cols].reshape(width, mixed)
                return jnp.dot(normed[s, i], matrix, preferred_element_type=F32)

            here = pl.ds(pl.multiple_of(zi * sub + at, 128), mixed)
            scales = iscale[:, here]
            inner = (product(1) * scales[1:2]) * (product(2) * scales[2:3])
            convolved = causal_taps(inner, mtaps[:, here])
            cols = pl.ds(pl.multiple_of(at, 128), mixed)
            gated[s, i, :, cols] = (product(0) * scales[0:1] * convolved).astype(BF16)
            return carry

        lax.fori_loop(0, 2 * (sub // mixed), step, 0)

    for s in range(seqs):
        mixer(s)
    gather_sent(MIX)
    arrive(C, [1])
    launch(E, [0])
    complete(B)
    for s in range(seqs):
        scatter_begin(MIX, s, order)
        scatter_x(MIX, s)
    arrive(E, [1])
    arrive(C, rest[:1])
    scatter_z(MIX, 0)
    arrive(E, rest[:1])
    arrive(C, rest[1:])
    for s in range(1, seqs):
        scatter_z(MIX, s)
    resid(0)
    arrive(E, rest[1:])
    gather_x(DOWN, 0)
    down_launch(True)
    for s in range(1, seqs):
        resid(s)
    down_launch(False)
    gather_done(DOWN, 0)
    normalize(0, gain2)
    complete(C)
    complete(E)

    def up(s):
        def activate(gate, val):
            return gate / (1.0 + jnp.exp(-gate)) * val

        def step(j, carry):
            i, t = j % 2, j // 2
            matrix = buf_c[:, :, lanes_at(t * 256, 256)].reshape(width, 256)
            both = jnp.dot(normed[s, i], matrix, preferred_element_type=F32)
            here = lanes_at((zi * second + t) * 128, 128)
            gate = causal_taps(both[:, :128] * uscale[0:1, here], ftaps[0, :, here])
            val = causal_taps(both[:, 128:] * uscale[1:2, here], ftaps[1, :, here])
            active[s, i, :, lanes_at(t * 128, 128)] = activate(gate, val).astype(BF16)
            return carry

        lax.fori_loop(0, 2 * full, step, 0)
        if odd:
            mid = slice(full * 128, full * 128 + 128)
            scale = join_halves(uscale[0:1, mid], uscale[1:2, mid], zi)
            taps = join_halves(ftaps[0, :, mid], ftaps[1, :, mid], zi)

            def last(i, carry):
                matrix = buf_c[:, :, full * 256 :].reshape(width, 128)
                both = jnp.dot(normed[s, i], matrix, preferred_element_type=F32)
                gate = causal_taps(both * scale, taps)
                values = activate(gate, pltpu.roll(gate, 64, 1))
                lanes = lax.broadcasted_iota(jnp.int32, values.shape, 1)
                active[s, i, :, mid] = jnp.where(lanes < 64, values, 0.0).astype(BF16)
                return carry

            lax.fori_loop(0, 2, last, 0)

    up(0)
    down_arrive(True)
    for s in range(1, seqs):
        gather_x(DOWN, s)
        gather_done(DOWN, s)
        normalize(s, gain2)
    down_arrive(False)
    scatter_sent(MIX)
    down_complete(True)
    for s in range(seqs):
        if s:
            up(s)
        scatter_begin(DOWN, s, order[:-1])
        scatter_x(DOWN, s)
    down_complete(False)
    for s in range(seqs):
        scatter_begin(DOWN, s, [0])
    for s in range(seqs):
        scatter_z(DOWN, s)
    for s in range(seqs):
        finish(s)

    gather_sent(DOWN)
    scatter_sent(DOWN)
    for g in range(8):
        for r in range(planes):
            to_row(g, r).wait_send()
            if r:
                to_plane(g, r).wait_send()


def on_device(
    n,
    n_tp,
    tokens,
    mix_gain,
    w_bgate,
    w_cgate,
    w_value,
    in_scale,
    mix_taps,
    w_mixout,
    mixout_scale,
    ffn_gain,
    w_upgate,
    w_upval,
    up_scale,
    ffn_taps,
    w_down,
    down_scale,
):
    seqs, length, own = tokens.shape
    width = own * n_tp
    part = w_bgate.shape[0]
    ff = w_upgate.shape[1]
    pad = -ff % 128
    ffp = ff + pad
    bw = w_mixout.shape[1]

    if pad:
        w_upgate, w_upval, up_scale, ffn_taps = (
            jnp.pad(x, [(0, 0)] * (x.ndim - 1) + [(0, pad)])
            for x in (w_upgate, w_upval, up_scale, ffn_taps)
        )
        w_down = jnp.pad(w_down, ((0, pad), (0, 0)))
    weights = (w_bgate, w_cgate, w_value, w_mixout, w_upgate, w_upval, w_down)
    planes, chips, sub = n // 2, n_tp // 2, own // 2
    full, odd = ffp // 128 // 2, ffp // 128 % 2
    hidden, down_rows = (full + odd) * 128, full * 128 + odd * 64
    vmem, dma = pltpu.VMEM, pltpu.SemaphoreType.DMA
    result = pl.pallas_call(
        functools.partial(layer_kernel, n, n_tp),
        out_shape=jax.ShapeDtypeStruct((seqs, length, own), BF16),
        in_specs=[pl.BlockSpec(memory_space=pltpu.VMEM)] * 9
        + [pl.BlockSpec(memory_space=pl.ANY)] * 7,
        out_specs=pl.BlockSpec(memory_space=pltpu.VMEM),
        scratch_shapes=[
            vmem((n, 8, bw), F32),
            vmem((n, part, 3 * sub), BF16),
            vmem((n, sub, bw), BF16),
            vmem((n, part, ffp), BF16),
            vmem((n, hidden, bw), BF16),
            vmem((part, 3 * sub), BF16),
            vmem((sub, bw), BF16),
            vmem((part, ffp), BF16),
            vmem((down_rows, bw), BF16),
        ]
        + [vmem(w.shape, F32) for w in weights]
        + [
            vmem((2, n_tp, seqs, length, own), BF16),
            vmem((seqs, 2, length, width), BF16),
            vmem((seqs, 2, length, sub), BF16),
            vmem((seqs, 2, length, hidden), BF16),
            vmem((chips, 2, seqs, 2, length, own), BF16),
            vmem((seqs, 2, length, own), BF16),
            vmem((2, chips, seqs, 2, length, own), BF16),
            vmem((2, chips - 1, seqs, 2, length, own), BF16),
            vmem((2, seqs, 2, length, own), BF16),
            dma((8, planes - 1)),
            dma((8, planes - 1)),
            dma((8, planes)),
            dma((8, planes)),
            dma((2, seqs)),
            dma((2, seqs)),
            dma((2, seqs, chips - 1, 2)),
            dma((2, seqs, chips - 1, 2)),
            dma((2, seqs, chips, 2)),
            dma((2, seqs, chips, 2)),
            dma((2, seqs)),
            dma((2, seqs)),
            dma((2, seqs, chips - 1)),
            dma((2, seqs, chips - 1)),
            dma((2, seqs, chips)),
            dma((2, seqs, chips)),
            dma((7,)),
        ],
        compiler_params=pltpu.CompilerParams(
            collective_id=0, has_side_effects=True, vmem_limit_bytes=67043328
        ),
        name="layer",
    )(
        tokens, mix_gain.reshape(1, width), ffn_gain.reshape(1, width),
        in_scale, mix_taps, up_scale, ffn_taps, mixout_scale, down_scale, *weights,
    )
    return result


def solution(mesh):
    in_specs = (
        P("fs", None, "tp"),
        P(),
        P("fs", "tp"),
        P("fs", "tp"),
        P("fs", "tp"),
        P(None, "tp"),
        P(None, "tp"),
        P("tp", "fs"),
        P(None, "fs"),
        P(),
        P("fs", "tp"),
        P("fs", "tp"),
        P(None, "tp"),
        P(None, None, "tp"),
        P("tp", "fs"),
        P(None, "fs"),
    )
    out_specs = P("fs", None, "tp")
    body = functools.partial(on_device, mesh.shape["fs"], mesh.shape["tp"])
    return jax.shard_map(body, mesh=mesh, in_specs=in_specs, out_specs=out_specs, check_vma=False)
```

```python
import functools

import jax
import jax.numpy as jnp
from jax import lax
from jax.experimental import pallas as pl
from jax.experimental.pallas import tpu as pltpu
from jax.sharding import PartitionSpec as P

EPS = 1e-06
MESH = pl.DeviceIdType.MESH
F32 = jnp.float32
BF16 = jnp.bfloat16
S, A, F, B, C, E, D, G = range(8)
MIX, DOWN = 0, 1


def shifted(values, by):
    rows = lax.broadcasted_iota(jnp.int32, values.shape, 0)
    return jnp.where(rows >= by, pltpu.roll(values, by, 0), 0.0)


def causal_taps(values, taps):
    return shifted(values, 2) * taps[0:1] + shifted(values, 1) * taps[1:2] + values * taps[2:3]


def join_halves(first, second, which):
    half = first.shape[-1] // 2
    lanes = lax.broadcasted_iota(jnp.int32, first.shape, 1)
    low = jnp.where(lanes < half, first, pltpu.roll(second, half, 1))
    high = jnp.where(lanes < half, pltpu.roll(first, half, 1), second)
    return jnp.where(which == 0, low, high)


def layer_kernel(
    n, n_tp, tok, gain1, gain2, iscale, mtaps, uscale, ftaps, mscale, dscale,
    w_bgate, w_cgate, w_value, w_mixout, w_upgate, w_upval, w_down, out,
    buf_s, buf_a, buf_b, buf_c, buf_d, st_a, st_b, st_c, st_d,
    f_bgate, f_cgate, f_value, f_mixout, f_upgate, f_upval, f_down,
    xg, normed, gated, active, parts, zparts, recv_core, recv_x, recv_z,
    wz_send, wz_recv, wy_send, wy_recv, ag_z_send, ag_z_recv, ag_x_send, ag_x_recv,
    ag_c_send, ag_c_recv, rs_z_send, rs_z_recv, rs_zz_send, rs_zz_recv, rs_x_send, rs_x_recv, rs_c_send, rs_c_recv,
    local_sem,
):
    fs, me = lax.axis_index("fs"), lax.axis_index("tp")
    seqs, length, own = tok.shape
    width = own * n_tp
    planes, chips = n // 2, n_tp // 2
    bpo = n // n_tp
    bw = own // bpo
    sub = own // 2
    y, zz = fs % 2, fs // 2
    zi = zz % 2
    inner = (zz + zz // 2) % 2
    other = 1 - zi
    x, c = me // 2, me % 2
    blocks = f_upgate.shape[1] // 128
    full, odd = blocks // 2, blocks % 2
    second = full + odd
    down_rows = full * 128 + odd * 64

    def plane(r):
        result, bit = 0, 1
        while bit < planes:
            digit = zz // bit % 2
            result = result + bit * ((1 - digit) if r & bit else digit)
            bit *= 2
        return result

    def tp_of(r, core):
        return (x + r) % chips * 2 + core

    def remote(src, dst, send, recv, where):
        return pltpu.make_async_remote_copy(
            src_ref=src, dst_ref=dst, send_sem=send, recv_sem=recv,
            device_id=where, device_id_type=MESH,
        )

    bufs = (buf_s, buf_a, buf_a, buf_b, buf_c, buf_c, buf_d, buf_d)
    stages = (None, st_a, st_a, st_b, st_c, st_c, st_d, st_d)
    half = buf_c.shape[1] // 2
    low, high = pl.ds(0, half), pl.ds(half, half)
    spans = {A: low, F: high, C: low, E: high}
    spans[D] = pl.ds(0, down_rows // 2)
    spans[G] = pl.ds(down_rows // 2, down_rows // 2)

    def piece(g, at):
        return bufs[g].at[at, spans[g]] if g in spans else bufs[g].at[at]

    def stage(g):
        return stages[g].at[spans[g]] if g in spans else stages[g]

    def to_plane(g, r):
        src = stage(g) if r % 2 and g != S else piece(g, fs)
        return remote(
            src, piece(g, fs), wz_send.at[g, r - 1], wz_recv.at[g, r - 1],
            {"fs": plane(r) * 2 + y},
        )

    def to_row(g, r):
        at = piece(g, plane(r) * 2 + y)
        return remote(at, at, wy_send.at[g, r], wy_recv.at[g, r], {"fs": fs + 1 - 2 * y})

    def launch(g, rs):
        for r in rs:
            if r:
                to_plane(g, r).start()
            else:
                to_row(g, 0).start()

    def arrive(g, rs):
        for r in rs:
            to_plane(g, r).wait_recv()
            to_row(g, r).start()

    def complete(g):
        for r in range(planes):
            to_row(g, r).wait_recv()

    across = range(1, planes)
    rest = list(across)[:0:-1]

    def ag_z(k, s, src=None):
        at = xg.at[zi, me, s]
        return remote(
            at if src is None else src, at, ag_z_send.at[k, s], ag_z_recv.at[k, s],
            {"fs": fs + 2 - 4 * zi},
        )

    def ag_x(k, s, r, i, src=None):
        at = xg.at[other if i else zi, me, s]
        return remote(
            at if src is None else src, at, ag_x_send.at[k, s, r - 1, i],
            ag_x_recv.at[k, s, r - 1, i], {"tp": tp_of(r, c)},
        )

    def ag_c(k, s, r, i, src=None):
        at = xg.at[other if i else zi, tp_of(chips - r, c), s]
        return remote(
            at if src is None else src, at, ag_c_send.at[k, s, r, i], ag_c_recv.at[k, s, r, i],
            {"tp": me + 1 - 2 * c},
        )

    def gather_own(k, s, src=None):
        ag_z(k, s, src).start()
        for r in range(1, chips):
            ag_x(k, s, r, 0, src).start()
        ag_c(k, s, 0, 0, src).start()

    def gather_z(k, s):
        ag_z(k, s).wait_recv()
        for r in range(1, chips):
            ag_x(k, s, r, 1).start()
        ag_c(k, s, 0, 1).start()

    def gather_x(k, s):
        for i in (0, 1):
            for r in range(1, chips):
                ag_x(k, s, r, i).wait_recv()
                ag_c(k, s, r, i).start()

    def gather_done(k, s):
        for i in (0, 1):
            for r in range(chips):
                ag_c(k, s, r, i).wait_recv()

    def gather_sent(k):
        for s in range(seqs):
            if k == MIX:
                ag_z(k, s).wait_send()
            for i in (0, 1):
                for r in range(1, chips):
                    ag_x(k, s, r, i).wait_send()
                for r in range(chips):
                    ag_c(k, s, r, i).wait_send()

    def rs_c(k, s, r):
        return remote(
            parts.at[r, 1, s], recv_core.at[k, r, s], rs_c_send.at[k, s, r],
            rs_c_recv.at[k, s, r], {"tp": me + 1 - 2 * c},
        )

    def rs_x(k, s, r):
        return remote(
            parts.at[r, 0, s], recv_x.at[k, r - 1, s], rs_x_send.at[k, s, r - 1],
            rs_x_recv.at[k, s, r - 1], {"tp": tp_of(r, c)},
        )

    def rs_z(k, s):
        src, dst = zparts.at[s, pl.ds(0, 2)], recv_z.at[k, s, pl.ds(0, 2)]
        if k == DOWN:
            src, dst = zparts.at[s, other], recv_z.at[k, s, 0]
        return remote(
            src, dst, rs_z_send.at[k, s], rs_z_recv.at[k, s], {"fs": fs + 2 - 4 * zi},
        )

    def products(k, s, r, side):
        owner = tp_of(r, 1 - c if side else c)
        source, held = ((gated, buf_b), (active, buf_d))[k]
        for i in (0, 1):
            for b in range(bpo):
                at = owner * bpo + b
                part = jnp.dot(source[s, i], held[at], preferred_element_type=F32)
                parts[r, side, s, i, :, b * bw : (b + 1) * bw] = (
                    part * buf_s[at, k : k + 1, :]
                ).astype(BF16)

    order = list(range(1, chips)) + [0]
    tile = 64

    def scatter_begin(k, s, rs):
        for r in rs:
            products(k, s, r, 1)
            rs_c(k, s, r).start()
        for r in rs:
            products(k, s, r, 0)

    def away(r):
        return plane(r) // 2 != x

    def each_down(test, do, rs):
        for r in rs:

            @pl.when(test(r))
            def _(r=r):
                for g in (D, G):
                    do(g, r)

    def down_launch(first):
        @pl.when(away(0) == first)
        def _():
            for r in [0, 1]:
                launch(D, [r])
                launch(G, [r])

            @pl.when(inner == 0)
            def _():
                down_across(rest)

    def down_across(rs):
        for r in rs:
            launch(D, [r])
            launch(G, [r])

    def down_arrive(first, rs):
        each_down(lambda r: away(r) == first, lambda g, r: arrive(g, [r]), rs)

    def down_complete(first):
        each_down(
            lambda r: away(r) == first, lambda g, r: to_row(g, r).wait_recv(), [0, 1] + rest
        )

    def scatter_x(k, s):
        for r in range(1, chips):
            rs_c(k, s, r).wait_recv()

            def step(j, carry, r=r):
                at = pl.ds(pl.multiple_of(j * tile, tile), tile)
                for i in (0, 1):
                    total = parts[r, 0, s, i, at, :].astype(F32)
                    total = total + recv_core[k, r, s, i, at, :].astype(F32)
                    parts[r, 0, s, i, at, :] = total.astype(BF16)
                return carry

            lax.fori_loop(0, length // tile, step, 0)
            rs_x(k, s, r).start()

    def quad(k, s, i, at):
        total = parts[0, 0, s, i, at, :].astype(F32) + recv_core[k, 0, s, i, at, :].astype(F32)
        for r in range(1, chips):
            total = total + recv_x[k, r - 1, s, i, at, :].astype(F32)
        return total

    def scatter_z(k, s):
        rs_c(k, s, 0).wait_recv()
        for r in range(1, chips):
            rs_x(k, s, r).wait_recv()

        def step(j, carry):
            at = pl.ds(pl.multiple_of(j * tile, tile), tile)
            for i in (0, 1) if k == MIX else (other,):
                zparts[s, i, at, :] = quad(k, s, i, at).astype(BF16)
            return carry

        lax.fori_loop(0, length // tile, step, 0)
        rs_z(k, s).start()

    def resid(s):
        rs_z(MIX, s).wait_recv()

        def step(j, carry):
            at = pl.ds(pl.multiple_of(j * tile, tile), tile)
            for i in (0, 1):
                total = zparts[s, i, at, :].astype(F32) + recv_z[MIX, s, i, at, :].astype(F32)
                xg[i, me, s, at, :] = (xg[i, me, s, at, :].astype(F32) + total).astype(BF16)
            return carry

        lax.fori_loop(0, length // tile, step, 0)
        for i in (0, 1):
            for r in range(1, chips):
                ag_x(DOWN, s, r, i).start()
            ag_c(DOWN, s, 0, i).start()

    def rs_zz(s, r):
        return remote(
            zparts.at[s, r], recv_z.at[DOWN, s, r], rs_zz_send.at[s, r], rs_zz_recv.at[s, r],
            {"fs": fs + 2 - 4 * zi},
        )

    def rs_zx(s, r):
        return remote(
            parts.at[r, 0, s, zi], recv_x.at[DOWN, r - 1, s, 0], rs_x_send.at[DOWN, s, r - 1],
            rs_x_recv.at[DOWN, s, r - 1], {"tp": tp_of(r, c)},
        )

    def turned_z(s, rs):
        for r in rs:
            rs_c(DOWN, s, r).wait_recv()

            def step(j, carry, r=r):
                at = pl.ds(pl.multiple_of(j * tile, tile), tile)

                def pair(i):
                    total = parts[r, 0, s, i, at, :].astype(F32)
                    return total + recv_core[DOWN, r, s, i, at, :].astype(F32)

                zparts[s, r, at, :] = pair(other).astype(BF16)
                parts[r, 0, s, zi, at, :] = pair(zi).astype(BF16)
                return carry

            lax.fori_loop(0, length // tile, step, 0)
            rs_zz(s, r).start()

    def turned_x(s):
        for r in range(1, chips):
            rs_zz(s, r).wait_recv()

            def step(j, carry, r=r):
                at = pl.ds(pl.multiple_of(j * tile, tile), tile)
                total = parts[r, 0, s, zi, at, :].astype(F32)
                total = total + recv_z[DOWN, s, r, at, :].astype(F32)
                parts[r, 0, s, zi, at, :] = total.astype(BF16)
                return carry

            lax.fori_loop(0, length // tile, step, 0)
            rs_zx(s, r).start()

    def turned_finish(s):
        rs_zz(s, 0).wait_recv()
        for r in range(1, chips):
            rs_zx(s, r).wait_recv()

        def step(j, carry):
            at = pl.ds(pl.multiple_of(j * tile, tile), tile)
            total = parts[0, 0, s, zi, at, :].astype(F32)
            total = total + recv_z[DOWN, s, 0, at, :].astype(F32)
            for r in range(1, chips):
                total = total + recv_x[DOWN, r - 1, s, 0, at, :].astype(F32)
            out[s, at, :] = (xg[zi, me, s, at, :].astype(F32) + total).astype(BF16)
            return carry

        lax.fori_loop(0, length // tile, step, 0)

    def finish(s):
        rs_z(DOWN, s).wait_recv()

        def step(j, carry):
            at = pl.ds(pl.multiple_of(j * tile, tile), tile)
            total = quad(DOWN, s, zi, at) + recv_z[DOWN, s, 0, at, :].astype(F32)
            out[s, at, :] = (xg[zi, me, s, at, :].astype(F32) + total).astype(BF16)
            return carry

        lax.fori_loop(0, length // tile, step, 0)

    def scatter_sent(k):
        for s in range(seqs):
            turned = k == DOWN and s % 2
            for r in range(chips):
                rs_c(k, s, r).wait_send()
                if turned:
                    rs_zz(s, r).wait_send()
                if r:
                    (rs_zx(s, r) if turned else rs_x(k, s, r)).wait_send()
            if not turned:
                rs_z(k, s).wait_send()

    barrier = pltpu.get_barrier_semaphore()
    peers = [{"fs": plane(r) * 2 + y} for r in across]
    peers += [{"fs": fs + 1 - 2 * y}, {"tp": me + 1 - 2 * c}]
    peers += [{"tp": tp_of(r, c)} for r in range(1, chips)]
    for peer in peers:
        pl.semaphore_signal(barrier, inc=1, device_id=peer, device_id_type=MESH)

    sources = (w_bgate, w_cgate, w_value, w_mixout, w_upgate, w_upval, w_down)
    floats = (f_bgate, f_cgate, f_value, f_mixout, f_upgate, f_upval, f_down)
    loads = [
        pltpu.make_async_copy(source, held, local_sem.at[i])
        for i, (source, held) in enumerate(zip(sources, floats))
    ]
    for copy in loads:
        copy.start()

    def cast_rows(rows, put):
        step_rows = 32

        def step(i, carry):
            put(i * step_rows, step_rows)
            return carry

        lax.fori_loop(0, rows // step_rows, step, 0)

    def rows_at(start, count):
        return pl.ds(pl.multiple_of(start, 32), count)

    def lanes_at(start, count):
        return pl.ds(pl.multiple_of(start, 128), count)

    def put_in(start, count):
        at = rows_at(start, count)
        for i, held in enumerate((f_bgate, f_cgate, f_value)):
            cols = slice(i * sub, (i + 1) * sub)
            buf_a[fs, at, cols] = held[at, lanes_at(zi * sub, sub)].astype(BF16)
            st_a[at, cols] = held[at, lanes_at(other * sub, sub)].astype(BF16)

    def put_mixout(start, count):
        at = rows_at(start, count)
        buf_b[fs, at, :] = f_mixout[rows_at(zi * sub + start, count), :].astype(BF16)
        st_b[at, :] = f_mixout[rows_at(other * sub + start, count), :].astype(BF16)

    def put_up(start, count):
        at = rows_at(start, count)
        for j in range(full):
            for i, held in enumerate((f_upgate, f_upval)):
                cols = slice(j * 256 + i * 128, j * 256 + i * 128 + 128)
                mine = lanes_at((zi * second + j) * 128, 128)
                theirs = lanes_at((other * second + j) * 128, 128)
                buf_c[fs, at, cols] = held[at, mine].astype(BF16)
                st_c[at, cols] = held[at, theirs].astype(BF16)
        if odd:
            mid = slice(full * 128, full * 128 + 128)
            cols = slice(full * 256, full * 256 + 128)
            gate, val = f_upgate[at, mid], f_upval[at, mid]
            buf_c[fs, at, cols] = join_halves(gate, val, zi).astype(BF16)
            st_c[at, cols] = join_halves(gate, val, other).astype(BF16)

    def put_down(start, count):
        at = rows_at(start, count)
        buf_d[fs, at, :] = f_down[rows_at(zi * second * 128 + start, count), :].astype(BF16)
        st_d[at, :] = f_down[rows_at(other * second * 128 + start, count), :].astype(BF16)

    def put_down_mid(start, count):
        base = full * 128
        at = rows_at(base + start, count)
        buf_d[fs, at, :] = f_down[rows_at(base + zi * 64 + start, count), :].astype(BF16)
        st_d[at, :] = f_down[rows_at(base + other * 64 + start, count), :].astype(BF16)

    buf_s[fs] = jnp.zeros(buf_s.shape[1:], F32)
    buf_s[fs, 0:1, :] = mscale[...]
    buf_s[fs, 1:2, :] = dscale[...]
    for i in range(3):
        loads[i].wait()
    cast_rows(f_bgate.shape[0], put_in)
    pl.semaphore_wait(barrier, len(peers))

    launch(S, range(planes))
    gather_own(MIX, 0, tok.at[0])
    for g in (A, F):
        launch(g, [0, 1])
    for s in range(1, seqs):
        gather_own(MIX, s, tok.at[s])
    for r in rest:
        launch(A, [r])
        launch(F, [r])
    xg[zi, me] = tok[...]
    loads[3].wait()
    cast_rows(sub, put_mixout)
    launch(B, [0, 1])
    launch(B, rest)
    for i in (4, 5, 6):
        loads[i].wait()
    cast_rows(f_upgate.shape[0], put_up)
    cast_rows(full * 128, put_down)
    if odd:
        cast_rows(64, put_down_mid)
        for at in range(n):
            buf_d[at, down_rows:, :] = jnp.zeros((64, bw), BF16)

    def normalize(s, gain):
        step_rows = 32

        def step(j, carry):
            at = pl.ds(pl.multiple_of(j * step_rows, step_rows), step_rows)
            for i in (0, 1):
                squares = jnp.zeros((step_rows, 1), F32)
                for t in range(n_tp):
                    values = xg[i, t, s, at, :].astype(F32)
                    squares = squares + jnp.sum(values * values, axis=-1, keepdims=True)
                factor = lax.rsqrt(squares * (1.0 / width) + EPS)
                for t in range(n_tp):
                    cols = slice(t * own, (t + 1) * own)
                    values = xg[i, t, s, at, :].astype(F32)
                    normed[s, i, at, cols] = (values * factor * gain[:, cols]).astype(BF16)
            return carry

        lax.fori_loop(0, length // step_rows, step, 0)

    arrive(S, across)
    gather_z(MIX, 0)
    arrive(A, rest[:1])
    arrive(A, [1])
    gather_x(MIX, 0)
    arrive(F, rest[:1])
    arrive(F, [1])
    arrive(A, rest[1:])
    arrive(F, rest[1:])
    for s in range(1, seqs):
        gather_z(MIX, s)
    gather_done(MIX, 0)
    normalize(0, gain1)
    launch(C, [1])
    arrive(B, across)
    for s in range(1, seqs):
        gather_x(MIX, s)
        gather_done(MIX, s)
        normalize(s, gain1)
    launch(E, [1])
    for r in rest:
        launch(C, [r])
        launch(E, [r])
    launch(C, [0])
    complete(S)
    complete(A)
    complete(F)

    mixed = min(256, sub)

    def mixer(s):
        def step(j, carry):
            i, at = j % 2, j // 2 * mixed

            def product(m):
                cols = pl.ds(pl.multiple_of(m * sub + at, 128), mixed)
                matrix = buf_a[:, :, cols].reshape(width, mixed)
                return jnp.dot(normed[s, i], matrix, preferred_element_type=F32)

            here = pl.ds(pl.multiple_of(zi * sub + at, 128), mixed)
            scales = iscale[:, here]
            inner = (product(1) * scales[1:2]) * (product(2) * scales[2:3])
            convolved = causal_taps(inner, mtaps[:, here])
            cols = pl.ds(pl.multiple_of(at, 128), mixed)
            gated[s, i, :, cols] = (product(0) * scales[0:1] * convolved).astype(BF16)
            return carry

        lax.fori_loop(0, 2 * (sub // mixed), step, 0)

    for s in range(seqs):
        mixer(s)
    gather_sent(MIX)
    arrive(C, [1])
    launch(E, [0])
    complete(B)
    for s in range(seqs):
        scatter_begin(MIX, s, order)
        scatter_x(MIX, s)
    arrive(E, [1])
    arrive(C, rest[:1])
    scatter_z(MIX, 0)
    arrive(E, rest[:1])
    for s in range(1, seqs):
        scatter_z(MIX, s)
    arrive(C, rest[1:])
    resid(0)
    pl.when(inner == 1)(lambda: down_across(rest[:1]))
    arrive(E, rest[1:])
    gather_x(DOWN, 0)
    down_launch(True)
    for s in range(1, seqs):
        resid(s)
    down_launch(False)
    gather_done(DOWN, 0)
    normalize(0, gain2)
    complete(C)
    complete(E)

    def up(s, first, count):
        def activate(gate, val):
            return gate / (1.0 + jnp.exp(-gate)) * val

        def step(j, carry):
            i, t = first + j % count, j // count
            matrix = buf_c[:, :, lanes_at(t * 256, 256)].reshape(width, 256)
            both = jnp.dot(normed[s, i], matrix, preferred_element_type=F32)
            here = lanes_at((zi * second + t) * 128, 128)
            gate = causal_taps(both[:, :128] * uscale[0:1, here], ftaps[0, :, here])
            val = causal_taps(both[:, 128:] * uscale[1:2, here], ftaps[1, :, here])
            active[s, i, :, lanes_at(t * 128, 128)] = activate(gate, val).astype(BF16)
            return carry

        lax.fori_loop(0, count * full, step, 0)
        if odd:
            mid = slice(full * 128, full * 128 + 128)
            scale = join_halves(uscale[0:1, mid], uscale[1:2, mid], zi)
            taps = join_halves(ftaps[0, :, mid], ftaps[1, :, mid], zi)

            def last(i, carry):
                matrix = buf_c[:, :, full * 256 :].reshape(width, 128)
                both = jnp.dot(normed[s, i], matrix, preferred_element_type=F32)
                gate = causal_taps(both * scale, taps)
                values = activate(gate, pltpu.roll(gate, 64, 1))
                lanes = lax.broadcasted_iota(jnp.int32, values.shape, 1)
                active[s, i, :, mid] = jnp.where(lanes < 64, values, 0.0).astype(BF16)
                return carry

            lax.fori_loop(first, first + count, last, 0)

    pl.when(inner == 1)(lambda: down_across(rest[1:]))
    up(0, 0, 2)
    soon, late = [1] + rest[:1], rest[1:]
    down_arrive(True, soon)
    for s in range(1, seqs):
        gather_x(DOWN, s)
        gather_done(DOWN, s)
        normalize(s, gain2)
    down_arrive(False, soon)
    for s in range(1, seqs):
        up(s, 0, 1)
    down_arrive(True, late)
    for s in range(1, seqs):
        up(s, 1, 1)
    down_arrive(False, late)
    scatter_sent(MIX)
    down_complete(True)
    far = order[:-1]
    for s in range(seqs):
        scatter_begin(DOWN, s, far)
        if s % 2:
            turned_z(s, far)
        else:
            scatter_x(DOWN, s)
    down_complete(False)
    for s in range(seqs):
        scatter_begin(DOWN, s, [0])
        if s % 2:
            turned_z(s, [0])
    for s in range(0, seqs, 2):
        scatter_z(DOWN, s)
    for s in range(1, seqs, 2):
        turned_x(s)
    for s in range(seqs):
        if s % 2:
            turned_finish(s)
        else:
            finish(s)

    gather_sent(DOWN)
    scatter_sent(DOWN)
    for g in range(8):
        for r in range(planes):
            to_row(g, r).wait_send()
            if r:
                to_plane(g, r).wait_send()


def on_device(
    n,
    n_tp,
    tokens,
    mix_gain,
    w_bgate,
    w_cgate,
    w_value,
    in_scale,
    mix_taps,
    w_mixout,
    mixout_scale,
    ffn_gain,
    w_upgate,
    w_upval,
    up_scale,
    ffn_taps,
    w_down,
    down_scale,
):
    seqs, length, own = tokens.shape
    width = own * n_tp
    part = w_bgate.shape[0]
    ff = w_upgate.shape[1]
    pad = -ff % 128
    ffp = ff + pad
    bw = w_mixout.shape[1]

    if pad:
        w_upgate, w_upval, up_scale, ffn_taps = (
            jnp.pad(x, [(0, 0)] * (x.ndim - 1) + [(0, pad)])
            for x in (w_upgate, w_upval, up_scale, ffn_taps)
        )
        w_down = jnp.pad(w_down, ((0, pad), (0, 0)))
    weights = (w_bgate, w_cgate, w_value, w_mixout, w_upgate, w_upval, w_down)
    planes, chips, sub = n // 2, n_tp // 2, own // 2
    full, odd = ffp // 128 // 2, ffp // 128 % 2
    hidden, down_rows = (full + odd) * 128, full * 128 + odd * 64
    vmem, dma = pltpu.VMEM, pltpu.SemaphoreType.DMA
    result = pl.pallas_call(
        functools.partial(layer_kernel, n, n_tp),
        out_shape=jax.ShapeDtypeStruct((seqs, length, own), BF16),
        in_specs=[pl.BlockSpec(memory_space=pltpu.VMEM)] * 9
        + [pl.BlockSpec(memory_space=pl.ANY)] * 7,
        out_specs=pl.BlockSpec(memory_space=pltpu.VMEM),
        scratch_shapes=[
            vmem((n, 8, bw), F32),
            vmem((n, part, 3 * sub), BF16),
            vmem((n, sub, bw), BF16),
            vmem((n, part, ffp), BF16),
            vmem((n, hidden, bw), BF16),
            vmem((part, 3 * sub), BF16),
            vmem((sub, bw), BF16),
            vmem((part, ffp), BF16),
            vmem((down_rows, bw), BF16),
        ]
        + [vmem(w.shape, F32) for w in weights]
        + [
            vmem((2, n_tp, seqs, length, own), BF16),
            vmem((seqs, 2, length, width), BF16),
            vmem((seqs, 2, length, sub), BF16),
            vmem((seqs, 2, length, hidden), BF16),
            vmem((chips, 2, seqs, 2, length, own), BF16),
            vmem((seqs, max(2, chips), length, own), BF16),
            vmem((2, chips, seqs, 2, length, own), BF16),
            vmem((2, chips - 1, seqs, 2, length, own), BF16),
            vmem((2, seqs, max(2, chips), length, own), BF16),
            dma((8, planes - 1)),
            dma((8, planes - 1)),
            dma((8, planes)),
            dma((8, planes)),
            dma((2, seqs)),
            dma((2, seqs)),
            dma((2, seqs, chips - 1, 2)),
            dma((2, seqs, chips - 1, 2)),
            dma((2, seqs, chips, 2)),
            dma((2, seqs, chips, 2)),
            dma((2, seqs)),
            dma((2, seqs)),
            dma((seqs, chips)),
            dma((seqs, chips)),
            dma((2, seqs, chips - 1)),
            dma((2, seqs, chips - 1)),
            dma((2, seqs, chips)),
            dma((2, seqs, chips)),
            dma((7,)),
        ],
        compiler_params=pltpu.CompilerParams(
            collective_id=0, has_side_effects=True, vmem_limit_bytes=67043328
        ),
        name="layer",
    )(
        tokens, mix_gain.reshape(1, width), ffn_gain.reshape(1, width),
        in_scale, mix_taps, up_scale, ffn_taps, mixout_scale, down_scale, *weights,
    )
    return result


def solution(mesh):
    in_specs = (
        P("fs", None, "tp"),
        P(),
        P("fs", "tp"),
        P("fs", "tp"),
        P("fs", "tp"),
        P(None, "tp"),
        P(None, "tp"),
        P("tp", "fs"),
        P(None, "fs"),
        P(),
        P("fs", "tp"),
        P("fs", "tp"),
        P(None, "tp"),
        P(None, None, "tp"),
        P("tp", "fs"),
        P(None, "fs"),
    )
    out_specs = P("fs", None, "tp")
    body = functools.partial(on_device, mesh.shape["fs"], mesh.shape["tp"])
    return jax.shard_map(body, mesh=mesh, in_specs=in_specs, out_specs=out_specs, check_vma=False)
```

```python
import functools

import jax
import jax.numpy as jnp
from jax import lax
from jax.experimental import pallas as pl
from jax.experimental.pallas import tpu as pltpu
from jax.sharding import PartitionSpec as P

EPS = 1e-06
MESH = pl.DeviceIdType.MESH
F32 = jnp.float32
BF16 = jnp.bfloat16
S, A, F, B, C, E, D, G = range(8)
MIX, DOWN = 0, 1


def shifted(values, by, count):
    length = values.shape[0] // count
    rows = lax.broadcasted_iota(jnp.int32, values.shape, 0)
    keep = rows >= by
    for start in range(length, values.shape[0], length):
        keep &= (rows < start) | (rows >= start + by)
    return jnp.where(keep, pltpu.roll(values, by, 0), 0.0)


def causal_taps(values, taps, count):
    later = values * taps[2:3]
    return shifted(values, 2, count) * taps[0:1] + shifted(values, 1, count) * taps[1:2] + later


def join_halves(first, second, which):
    half = first.shape[-1] // 2
    lanes = lax.broadcasted_iota(jnp.int32, first.shape, 1)
    low = jnp.where(lanes < half, first, pltpu.roll(second, half, 1))
    high = jnp.where(lanes < half, pltpu.roll(first, half, 1), second)
    return jnp.where(which == 0, low, high)


def layer_kernel(
    n, n_tp, tok, gain1, gain2, iscale, mtaps, uscale, ftaps, mscale, dscale,
    w_bgate, w_cgate, w_value, w_mixout, w_upgate, w_upval, w_down, out,
    buf_s, buf_a, buf_b, buf_c, buf_d, st_a, st_b, st_c, st_d,
    f_bgate, f_cgate, f_value, f_mixout, f_upgate, f_upval, f_down,
    xg, normed, gated, active, parts, zparts, recv_core, recv_x, recv_z,
    wz_send, wz_recv, wy_send, wy_recv, ag_z_send, ag_z_recv, ag_x_send, ag_x_recv,
    ag_c_send, ag_c_recv, rs_z_send, rs_z_recv, rs_zz_send, rs_zz_recv, rs_x_send, rs_x_recv, rs_c_send, rs_c_recv,
    local_sem,
):
    fs, me = lax.axis_index("fs"), lax.axis_index("tp")
    seqs, length, own = tok.shape
    width = own * n_tp
    planes, chips = n // 2, n_tp // 2
    bpo = n // n_tp
    bw = own // bpo
    sub = own // 2
    y, zz = fs % 2, fs // 2
    zi = zz % 2
    inner = (zz + zz // 2) % 2
    other = 1 - zi
    x, c = me // 2, me % 2
    blocks = f_upgate.shape[1] // 128
    full, odd = blocks // 2, blocks % 2
    second = full + odd
    down_rows = full * 128 + odd * 64

    def plane(r):
        result, bit = 0, 1
        while bit < planes:
            digit = zz // bit % 2
            result = result + bit * ((1 - digit) if r & bit else digit)
            bit *= 2
        return result

    def tp_of(r, core):
        return (x + r) % chips * 2 + core

    def remote(src, dst, send, recv, where):
        return pltpu.make_async_remote_copy(
            src_ref=src, dst_ref=dst, send_sem=send, recv_sem=recv,
            device_id=where, device_id_type=MESH,
        )

    bufs = (buf_s, buf_a, buf_a, buf_b, buf_c, buf_c, buf_d, buf_d)
    stages = (None, st_a, st_a, st_b, st_c, st_c, st_d, st_d)
    half = buf_c.shape[1] // 2
    low, high = pl.ds(0, half), pl.ds(half, half)
    spans = {A: low, F: high, C: low, E: high}
    spans[D] = pl.ds(0, down_rows // 2)
    spans[G] = pl.ds(down_rows // 2, down_rows // 2)

    def piece(g, at):
        return bufs[g].at[at, spans[g]] if g in spans else bufs[g].at[at]

    def stage(g):
        return stages[g].at[spans[g]] if g in spans else stages[g]

    def to_plane(g, r):
        src = stage(g) if r % 2 and g != S else piece(g, fs)
        return remote(
            src, piece(g, fs), wz_send.at[g, r - 1], wz_recv.at[g, r - 1],
            {"fs": plane(r) * 2 + y},
        )

    def to_row(g, r):
        at = piece(g, plane(r) * 2 + y)
        return remote(at, at, wy_send.at[g, r], wy_recv.at[g, r], {"fs": fs + 1 - 2 * y})

    def launch(g, rs):
        for r in rs:
            if r:
                to_plane(g, r).start()
            else:
                to_row(g, 0).start()

    def arrive(g, rs):
        for r in rs:
            to_plane(g, r).wait_recv()
            to_row(g, r).start()

    def complete(g):
        for r in range(planes):
            to_row(g, r).wait_recv()

    across = range(1, planes)
    rest = list(across)[:0:-1]

    def ag_z(k, s, src=None):
        at = xg.at[zi, me, s]
        return remote(
            at if src is None else src, at, ag_z_send.at[k, s], ag_z_recv.at[k, s],
            {"fs": fs + 2 - 4 * zi},
        )

    def ag_x(k, s, r, i, src=None):
        at = xg.at[other if i else zi, me, s]
        return remote(
            at if src is None else src, at, ag_x_send.at[k, s, r - 1, i],
            ag_x_recv.at[k, s, r - 1, i], {"tp": tp_of(r, c)},
        )

    def ag_c(k, s, r, i, src=None):
        at = xg.at[other if i else zi, tp_of(chips - r, c), s]
        return remote(
            at if src is None else src, at, ag_c_send.at[k, s, r, i], ag_c_recv.at[k, s, r, i],
            {"tp": me + 1 - 2 * c},
        )

    def gather_own(k, s, src=None):
        ag_z(k, s, src).start()
        for r in range(1, chips):
            ag_x(k, s, r, 0, src).start()
        ag_c(k, s, 0, 0, src).start()

    def gather_z(k, s):
        ag_z(k, s).wait_recv()
        for r in range(1, chips):
            ag_x(k, s, r, 1).start()
        ag_c(k, s, 0, 1).start()

    def gather_x(k, s):
        for i in (0, 1):
            for r in range(1, chips):
                ag_x(k, s, r, i).wait_recv()
                ag_c(k, s, r, i).start()

    def gather_done(k, s):
        for i in (0, 1):
            for r in range(chips):
                ag_c(k, s, r, i).wait_recv()

    def gather_sent(k):
        for s in range(seqs):
            if k == MIX:
                ag_z(k, s).wait_send()
            for i in (0, 1):
                for r in range(1, chips):
                    ag_x(k, s, r, i).wait_send()
                for r in range(chips):
                    ag_c(k, s, r, i).wait_send()

    def rs_c(k, s, r):
        return remote(
            parts.at[r, 1, s], recv_core.at[k, r, s], rs_c_send.at[k, s, r],
            rs_c_recv.at[k, s, r], {"tp": me + 1 - 2 * c},
        )

    def rs_x(k, s, r, j):
        i = zi if j else other
        return remote(
            parts.at[r, 0, s, i], recv_x.at[k, r - 1, s, i], rs_x_send.at[k, s, r - 1, j],
            rs_x_recv.at[k, s, r - 1, j], {"tp": tp_of(r, c)},
        )

    def rs_z(k, s):
        src, dst = zparts.at[s, pl.ds(0, 2)], recv_z.at[k, s, pl.ds(0, 2)]
        if k == DOWN:
            src, dst = zparts.at[s, other], recv_z.at[k, s, 0]
        return remote(
            src, dst, rs_z_send.at[k, s], rs_z_recv.at[k, s], {"fs": fs + 2 - 4 * zi},
        )

    def products(k, s, r, side):
        owner = tp_of(r, 1 - c if side else c)
        source, held = ((gated, buf_b), (active, buf_d))[k]
        for b in range(bpo):
            at = owner * bpo + b
            lines = source[s].reshape(2 * length, source.shape[-1])
            part = jnp.dot(lines, held[at], preferred_element_type=F32)
            part = (part * buf_s[at, k : k + 1, :]).astype(BF16)
            parts[r, side, s, :, :, b * bw : (b + 1) * bw] = part.reshape(2, length, bw)

    order = list(range(1, chips)) + [0]
    tile = 64

    def scatter_begin(k, s, rs):
        for r in rs:
            products(k, s, r, 1)
            rs_c(k, s, r).start()
        for r in rs:
            products(k, s, r, 0)

    def away(r):
        return plane(r) // 2 != x

    def each_down(test, do, rs):
        for r in rs:

            @pl.when(test(r))
            def _(r=r):
                for g in (D, G):
                    do(g, r)

    def down_launch(first):
        @pl.when(away(0) == first)
        def _():
            down_across([1])

            @pl.when(inner == 0)
            def _():
                down_across(rest)

            if not first:
                pl.when(inner == 1)(lambda: down_across(rest))

    def down_across(rs):
        for r in rs:
            launch(D, [r])
            launch(G, [r])

    def down_arrive(first, rs):
        each_down(lambda r: away(r) == first, lambda g, r: arrive(g, [r]), rs)

    def down_complete(first):
        each_down(
            lambda r: away(r) == first, lambda g, r: to_row(g, r).wait_recv(), [0, 1] + rest
        )

    def scatter_x(k, s):
        for r in range(1, chips):
            rs_c(k, s, r).wait_recv()
            for part, i in enumerate((other, zi)):

                def step(j, carry, r=r, i=i):
                    at = pl.ds(pl.multiple_of(j * tile, tile), tile)
                    total = parts[r, 0, s, i, at, :].astype(F32)
                    total = total + recv_core[k, r, s, i, at, :].astype(F32)
                    parts[r, 0, s, i, at, :] = total.astype(BF16)
                    return carry

                lax.fori_loop(0, length // tile, step, 0)
                rs_x(k, s, r, part).start()

    def quad(k, s, i, at):
        total = parts[0, 0, s, i, at, :].astype(F32) + recv_core[k, 0, s, i, at, :].astype(F32)
        for r in range(1, chips):
            total = total + recv_x[k, r - 1, s, i, at, :].astype(F32)
        return total

    def scatter_z(k, s):
        rs_c(k, s, 0).wait_recv()
        for r in range(1, chips):
            rs_x(k, s, r, 0).wait_recv()
            if k == MIX:
                rs_x(k, s, r, 1).wait_recv()

        def step(j, carry):
            at = pl.ds(pl.multiple_of(j * tile, tile), tile)
            for i in (0, 1) if k == MIX else (other,):
                zparts[s, i, at, :] = quad(k, s, i, at).astype(BF16)
            return carry

        lax.fori_loop(0, length // tile, step, 0)
        rs_z(k, s).start()

    def resid(s):
        rs_z(MIX, s).wait_recv()

        def step(j, carry):
            at = pl.ds(pl.multiple_of(j * tile, tile), tile)
            for i in (0, 1):
                total = zparts[s, i, at, :].astype(F32) + recv_z[MIX, s, i, at, :].astype(F32)
                xg[i, me, s, at, :] = (xg[i, me, s, at, :].astype(F32) + total).astype(BF16)
            return carry

        lax.fori_loop(0, length // tile, step, 0)
        for i in (0, 1):
            for r in range(1, chips):
                ag_x(DOWN, s, r, i).start()
            ag_c(DOWN, s, 0, i).start()

    def rs_zz(s, r):
        return remote(
            zparts.at[s, r], recv_z.at[DOWN, s, r], rs_zz_send.at[s, r], rs_zz_recv.at[s, r],
            {"fs": fs + 2 - 4 * zi},
        )

    def rs_zx(s, r):
        return remote(
            parts.at[r, 0, s, zi], recv_x.at[DOWN, r - 1, s, 0], rs_x_send.at[DOWN, s, r - 1, 0],
            rs_x_recv.at[DOWN, s, r - 1, 0], {"tp": tp_of(r, c)},
        )

    def turned_z(s, rs):
        for r in rs:
            rs_c(DOWN, s, r).wait_recv()

            def step(j, carry, r=r):
                at = pl.ds(pl.multiple_of(j * tile, tile), tile)

                def pair(i):
                    total = parts[r, 0, s, i, at, :].astype(F32)
                    return total + recv_core[DOWN, r, s, i, at, :].astype(F32)

                zparts[s, r, at, :] = pair(other).astype(BF16)
                parts[r, 0, s, zi, at, :] = pair(zi).astype(BF16)
                return carry

            lax.fori_loop(0, length // tile, step, 0)
            rs_zz(s, r).start()

    def turned_x(s):
        for r in range(1, chips):
            rs_zz(s, r).wait_recv()

            def step(j, carry, r=r):
                at = pl.ds(pl.multiple_of(j * tile, tile), tile)
                total = parts[r, 0, s, zi, at, :].astype(F32)
                total = total + recv_z[DOWN, s, r, at, :].astype(F32)
                parts[r, 0, s, zi, at, :] = total.astype(BF16)
                return carry

            lax.fori_loop(0, length // tile, step, 0)
            rs_zx(s, r).start()

    def turned_finish(s):
        rs_zz(s, 0).wait_recv()
        for r in range(1, chips):
            rs_zx(s, r).wait_recv()

        def step(j, carry):
            at = pl.ds(pl.multiple_of(j * tile, tile), tile)
            total = parts[0, 0, s, zi, at, :].astype(F32)
            total = total + recv_z[DOWN, s, 0, at, :].astype(F32)
            for r in range(1, chips):
                total = total + recv_x[DOWN, r - 1, s, 0, at, :].astype(F32)
            out[s, at, :] = (xg[zi, me, s, at, :].astype(F32) + total).astype(BF16)
            return carry

        lax.fori_loop(0, length // tile, step, 0)

    def finish(s):
        rs_z(DOWN, s).wait_recv()
        for r in range(1, chips):
            rs_x(DOWN, s, r, 1).wait_recv()

        def step(j, carry):
            at = pl.ds(pl.multiple_of(j * tile, tile), tile)
            total = quad(DOWN, s, zi, at) + recv_z[DOWN, s, 0, at, :].astype(F32)
            out[s, at, :] = (xg[zi, me, s, at, :].astype(F32) + total).astype(BF16)
            return carry

        lax.fori_loop(0, length // tile, step, 0)

    def scatter_sent(k):
        for s in range(seqs):
            turned = k == DOWN and s % 2
            for r in range(chips):
                rs_c(k, s, r).wait_send()
                if turned:
                    rs_zz(s, r).wait_send()
                if r and turned:
                    rs_zx(s, r).wait_send()
                elif r:
                    for j in (0, 1):
                        rs_x(k, s, r, j).wait_send()
            if not turned:
                rs_z(k, s).wait_send()

    barrier = pltpu.get_barrier_semaphore()
    peers = [{"fs": plane(r) * 2 + y} for r in across]
    peers += [{"fs": fs + 1 - 2 * y}, {"tp": me + 1 - 2 * c}]
    peers += [{"tp": tp_of(r, c)} for r in range(1, chips)]
    for peer in peers:
        pl.semaphore_signal(barrier, inc=1, device_id=peer, device_id_type=MESH)

    sources = (w_bgate, w_cgate, w_value, w_mixout, w_upgate, w_upval, w_down)
    floats = (f_bgate, f_cgate, f_value, f_mixout, f_upgate, f_upval, f_down)
    loads = [
        pltpu.make_async_copy(source, held, local_sem.at[i])
        for i, (source, held) in enumerate(zip(sources, floats))
    ]
    for copy in loads:
        copy.start()

    def cast_rows(rows, put):
        step_rows = 32

        def step(i, carry):
            put(i * step_rows, step_rows)
            return carry

        lax.fori_loop(0, rows // step_rows, step, 0)

    def rows_at(start, count):
        return pl.ds(pl.multiple_of(start, 32), count)

    def lanes_at(start, count):
        return pl.ds(pl.multiple_of(start, 128), count)

    def put_in(start, count):
        at = rows_at(start, count)
        for i, held in enumerate((f_bgate, f_cgate, f_value)):
            cols = slice(i * sub, (i + 1) * sub)
            buf_a[fs, at, cols] = held[at, lanes_at(zi * sub, sub)].astype(BF16)
            st_a[at, cols] = held[at, lanes_at(other * sub, sub)].astype(BF16)

    def put_mixout(start, count):
        at = rows_at(start, count)
        buf_b[fs, at, :] = f_mixout[rows_at(zi * sub + start, count), :].astype(BF16)
        st_b[at, :] = f_mixout[rows_at(other * sub + start, count), :].astype(BF16)

    def put_up(start, count):
        at = rows_at(start, count)
        for j in range(full):
            for i, held in enumerate((f_upgate, f_upval)):
                cols = slice(j * 256 + i * 128, j * 256 + i * 128 + 128)
                mine = lanes_at((zi * second + j) * 128, 128)
                theirs = lanes_at((other * second + j) * 128, 128)
                buf_c[fs, at, cols] = held[at, mine].astype(BF16)
                st_c[at, cols] = held[at, theirs].astype(BF16)
        if odd:
            mid = slice(full * 128, full * 128 + 128)
            cols = slice(full * 256, full * 256 + 128)
            gate, val = f_upgate[at, mid], f_upval[at, mid]
            buf_c[fs, at, cols] = join_halves(gate, val, zi).astype(BF16)
            st_c[at, cols] = join_halves(gate, val, other).astype(BF16)

    def put_down(start, count):
        at = rows_at(start, count)
        buf_d[fs, at, :] = f_down[rows_at(zi * second * 128 + start, count), :].astype(BF16)
        st_d[at, :] = f_down[rows_at(other * second * 128 + start, count), :].astype(BF16)

    def put_down_mid(start, count):
        base = full * 128
        at = rows_at(base + start, count)
        buf_d[fs, at, :] = f_down[rows_at(base + zi * 64 + start, count), :].astype(BF16)
        st_d[at, :] = f_down[rows_at(base + other * 64 + start, count), :].astype(BF16)

    buf_s[fs] = jnp.zeros(buf_s.shape[1:], F32)
    buf_s[fs, 0:1, :] = mscale[...]
    buf_s[fs, 1:2, :] = dscale[...]
    for i in range(3):
        loads[i].wait()
    cast_rows(f_bgate.shape[0], put_in)
    pl.semaphore_wait(barrier, len(peers))

    launch(S, range(planes))
    gather_own(MIX, 0, tok.at[0])
    for g in (A, F):
        launch(g, [0, 1])
    for s in range(1, seqs):
        gather_own(MIX, s, tok.at[s])
    for r in rest:
        launch(A, [r])
        launch(F, [r])
    xg[zi, me] = tok[...]
    loads[3].wait()
    cast_rows(sub, put_mixout)
    launch(B, [0, 1])
    launch(B, rest)
    for i in (4, 5, 6):
        loads[i].wait()
    cast_rows(f_upgate.shape[0], put_up)
    cast_rows(full * 128, put_down)
    if odd:
        cast_rows(64, put_down_mid)
        for at in range(n):
            buf_d[at, down_rows:, :] = jnp.zeros((64, bw), BF16)

    def normalize(s, gain):
        step_rows = 32

        def step(j, carry):
            at = pl.ds(pl.multiple_of(j * step_rows, step_rows), step_rows)
            for i in (0, 1):
                squares = jnp.zeros((step_rows, 1), F32)
                for t in range(n_tp):
                    values = xg[i, t, s, at, :].astype(F32)
                    squares = squares + jnp.sum(values * values, axis=-1, keepdims=True)
                factor = lax.rsqrt(squares * (1.0 / width) + EPS)
                for t in range(n_tp):
                    cols = slice(t * own, (t + 1) * own)
                    values = xg[i, t, s, at, :].astype(F32)
                    normed[s, i, at, cols] = (values * factor * gain[:, cols]).astype(BF16)
            return carry

        lax.fori_loop(0, length // step_rows, step, 0)

    arrive(S, across)
    gather_z(MIX, 0)
    arrive(A, rest[:1])
    arrive(A, [1])
    gather_x(MIX, 0)
    arrive(F, rest[:1])
    arrive(F, [1])
    arrive(A, rest[1:])
    arrive(F, rest[1:])
    for s in range(1, seqs):
        gather_z(MIX, s)
    gather_done(MIX, 0)
    normalize(0, gain1)
    launch(C, [1])
    arrive(B, across)
    for s in range(1, seqs):
        gather_x(MIX, s)
        gather_done(MIX, s)
        normalize(s, gain1)
    launch(E, [1])
    for r in rest:
        launch(C, [r])
        launch(E, [r])
    launch(C, [0])
    complete(S)
    complete(A)
    complete(F)

    mixed = min(256, sub)

    def both_of(s):
        return normed[s].reshape(2 * length, width)

    def mixer(s):
        def step(j, carry):
            i, at = j % 2, j // 2 * mixed

            def product(m):
                cols = pl.ds(pl.multiple_of(m * sub + at, 128), mixed)
                matrix = buf_a[:, :, cols].reshape(width, mixed)
                return jnp.dot(normed[s, i], matrix, preferred_element_type=F32)

            here = pl.ds(pl.multiple_of(zi * sub + at, 128), mixed)
            scales = iscale[:, here]
            inner = (product(1) * scales[1:2]) * (product(2) * scales[2:3])
            convolved = causal_taps(inner, mtaps[:, here], 1)
            cols = pl.ds(pl.multiple_of(at, 128), mixed)
            gated[s, i, :, cols] = (product(0) * scales[0:1] * convolved).astype(BF16)
            return carry

        lax.fori_loop(0, 2 * (sub // mixed), step, 0)

    for s in range(seqs):
        mixer(s)
    gather_sent(MIX)
    arrive(C, [1])
    launch(E, [0])
    complete(B)
    for s in range(seqs):
        scatter_begin(MIX, s, order)
        scatter_x(MIX, s)
    arrive(E, [1])
    arrive(C, rest[:1])
    scatter_z(MIX, 0)
    arrive(E, rest[:1])
    for s in range(1, seqs):
        scatter_z(MIX, s)
    arrive(C, rest[1:])
    resid(0)
    pl.when((inner == 1) & away(0))(lambda: down_across(rest[:1]))
    arrive(E, rest[1:])
    down_across([0])
    gather_x(DOWN, 0)
    down_launch(True)
    for s in range(1, seqs):
        resid(s)
    gather_done(DOWN, 0)
    normalize(0, gain2)
    complete(C)
    complete(E)

    def up(s, first, last):
        def activate(gate, val):
            return gate / (1.0 + jnp.exp(-gate)) * val

        def step(t, carry):
            matrix = buf_c[:, :, lanes_at(t * 256, 256)].reshape(width, 256)
            both = jnp.dot(both_of(s), matrix, preferred_element_type=F32)
            here = lanes_at((zi * second + t) * 128, 128)
            gate = causal_taps(both[:, :128] * uscale[0:1, here], ftaps[:, 0, here], 2)
            val = causal_taps(both[:, 128:] * uscale[1:2, here], ftaps[:, 1, here], 2)
            values = activate(gate, val).astype(BF16)
            active[s, :, :, lanes_at(t * 128, 128)] = values.reshape(2, length, 128)
            return carry

        lax.fori_loop(first, last, step, 0)
        if odd and last == full:
            mid = slice(full * 128, full * 128 + 128)
            scale = join_halves(uscale[0:1, mid], uscale[1:2, mid], zi)
            taps = join_halves(ftaps[:, 0, mid], ftaps[:, 1, mid], zi)
            matrix = buf_c[:, :, full * 256 :].reshape(width, 128)
            both = jnp.dot(both_of(s), matrix, preferred_element_type=F32)
            gate = causal_taps(both * scale, taps, 2)
            values = activate(gate, pltpu.roll(gate, 64, 1))
            lanes = lax.broadcasted_iota(jnp.int32, values.shape, 1)
            values = jnp.where(lanes < 64, values, 0.0).astype(BF16)
            active[s, :, :, mid] = values.reshape(2, length, 128)

    pl.when((inner == 1) & away(0))(lambda: down_across(rest[1:]))
    up(0, 0, full)
    down_launch(False)
    soon, late = [1] + rest[:1], rest[1:]
    down_arrive(True, soon)
    for s in range(1, seqs):
        gather_x(DOWN, s)
        gather_done(DOWN, s)
        normalize(s, gain2)
    down_arrive(True, late)
    for s in range(1, seqs):
        up(s, 0, full // 2)
    down_arrive(False, soon)
    for s in range(1, seqs):
        up(s, full // 2, full)
    scatter_sent(MIX)
    down_complete(True)
    far = order[:-1]
    for s in range(seqs):
        scatter_begin(DOWN, s, far)
        if s % 2:
            turned_z(s, far)
        else:
            scatter_x(DOWN, s)
    down_arrive(False, late)
    down_complete(False)
    for s in range(0, seqs, 2):
        scatter_begin(DOWN, s, [0])
        scatter_z(DOWN, s)
    for s in range(1, seqs, 2):
        scatter_begin(DOWN, s, [0])
        turned_z(s, [0])
    for s in range(1, seqs, 2):
        turned_x(s)
    for s in range(seqs):
        if s % 2:
            turned_finish(s)
        else:
            finish(s)

    gather_sent(DOWN)
    scatter_sent(DOWN)
    for g in range(8):
        for r in range(planes):
            to_row(g, r).wait_send()
            if r:
                to_plane(g, r).wait_send()


def on_device(
    n,
    n_tp,
    tokens,
    mix_gain,
    w_bgate,
    w_cgate,
    w_value,
    in_scale,
    mix_taps,
    w_mixout,
    mixout_scale,
    ffn_gain,
    w_upgate,
    w_upval,
    up_scale,
    ffn_taps,
    w_down,
    down_scale,
):
    seqs, length, own = tokens.shape
    width = own * n_tp
    part = w_bgate.shape[0]
    ff = w_upgate.shape[1]
    pad = -ff % 128
    ffp = ff + pad
    bw = w_mixout.shape[1]

    if pad:
        w_upgate, w_upval, up_scale, ffn_taps = (
            jnp.pad(x, [(0, 0)] * (x.ndim - 1) + [(0, pad)])
            for x in (w_upgate, w_upval, up_scale, ffn_taps)
        )
        w_down = jnp.pad(w_down, ((0, pad), (0, 0)))
    weights = (w_bgate, w_cgate, w_value, w_mixout, w_upgate, w_upval, w_down)
    planes, chips, sub = n // 2, n_tp // 2, own // 2
    full, odd = ffp // 128 // 2, ffp // 128 % 2
    hidden, down_rows = (full + odd) * 128, full * 128 + odd * 64
    vmem, dma = pltpu.VMEM, pltpu.SemaphoreType.DMA
    result = pl.pallas_call(
        functools.partial(layer_kernel, n, n_tp),
        out_shape=jax.ShapeDtypeStruct((seqs, length, own), BF16),
        in_specs=[pl.BlockSpec(memory_space=pltpu.VMEM)] * 9
        + [pl.BlockSpec(memory_space=pl.ANY)] * 7,
        out_specs=pl.BlockSpec(memory_space=pltpu.VMEM),
        scratch_shapes=[
            vmem((n, 8, bw), F32),
            vmem((n, part, 3 * sub), BF16),
            vmem((n, sub, bw), BF16),
            vmem((n, part, ffp), BF16),
            vmem((n, hidden, bw), BF16),
            vmem((part, 3 * sub), BF16),
            vmem((sub, bw), BF16),
            vmem((part, ffp), BF16),
            vmem((down_rows, bw), BF16),
        ]
        + [vmem(w.shape, F32) for w in weights]
        + [
            vmem((2, n_tp, seqs, length, own), BF16),
            vmem((seqs, 2, length, width), BF16),
            vmem((seqs, 2, length, sub), BF16),
            vmem((seqs, 2, length, hidden), BF16),
            vmem((chips, 2, seqs, 2, length, own), BF16),
            vmem((seqs, max(2, chips), length, own), BF16),
            vmem((2, chips, seqs, 2, length, own), BF16),
            vmem((2, chips - 1, seqs, 2, length, own), BF16),
            vmem((2, seqs, max(2, chips), length, own), BF16),
            dma((8, planes - 1)),
            dma((8, planes - 1)),
            dma((8, planes)),
            dma((8, planes)),
            dma((2, seqs)),
            dma((2, seqs)),
            dma((2, seqs, chips - 1, 2)),
            dma((2, seqs, chips - 1, 2)),
            dma((2, seqs, chips, 2)),
            dma((2, seqs, chips, 2)),
            dma((2, seqs)),
            dma((2, seqs)),
            dma((seqs, chips)),
            dma((seqs, chips)),
            dma((2, seqs, chips - 1, 2)),
            dma((2, seqs, chips - 1, 2)),
            dma((2, seqs, chips)),
            dma((2, seqs, chips)),
            dma((7,)),
        ],
        compiler_params=pltpu.CompilerParams(
            collective_id=0, has_side_effects=True, vmem_limit_bytes=67043328
        ),
        name="layer",
    )(
        tokens, mix_gain.reshape(1, width), ffn_gain.reshape(1, width),
        in_scale, mix_taps, up_scale, ffn_taps.transpose(1, 0, 2), mixout_scale, down_scale, *weights,
    )
    return result


def solution(mesh):
    in_specs = (
        P("fs", None, "tp"),
        P(),
        P("fs", "tp"),
        P("fs", "tp"),
        P("fs", "tp"),
        P(None, "tp"),
        P(None, "tp"),
        P("tp", "fs"),
        P(None, "fs"),
        P(),
        P("fs", "tp"),
        P("fs", "tp"),
        P(None, "tp"),
        P(None, None, "tp"),
        P("tp", "fs"),
        P(None, "fs"),
    )
    out_specs = P("fs", None, "tp")
    body = functools.partial(on_device, mesh.shape["fs"], mesh.shape["tp"])
    return jax.shard_map(body, mesh=mesh, in_specs=in_specs, out_specs=out_specs, check_vma=False)
```

```python
import functools

import jax
import jax.numpy as jnp
from jax import lax
from jax.experimental import pallas as pl
from jax.experimental.pallas import tpu as pltpu
from jax.sharding import PartitionSpec as P

EPS = 1e-06
MESH = pl.DeviceIdType.MESH
F32 = jnp.float32
BF16 = jnp.bfloat16
S, A, F, B, C, E, D, G = range(8)
MIX, DOWN = 0, 1


def shifted(values, by, count):
    length = values.shape[0] // count
    rows = lax.broadcasted_iota(jnp.int32, values.shape, 0)
    keep = rows >= by
    for start in range(length, values.shape[0], length):
        keep &= (rows < start) | (rows >= start + by)
    return jnp.where(keep, pltpu.roll(values, by, 0), 0.0)


def causal_taps(values, taps, count):
    later = values * taps[2:3]
    return shifted(values, 2, count) * taps[0:1] + shifted(values, 1, count) * taps[1:2] + later


def join_halves(first, second, which):
    half = first.shape[-1] // 2
    lanes = lax.broadcasted_iota(jnp.int32, first.shape, 1)
    low = jnp.where(lanes < half, first, pltpu.roll(second, half, 1))
    high = jnp.where(lanes < half, pltpu.roll(first, half, 1), second)
    return jnp.where(which == 0, low, high)


def layer_kernel(
    n, n_tp, tok, gain1, gain2, iscale, mtaps, uscale, ftaps, mscale, dscale,
    w_bgate, w_cgate, w_value, w_mixout, w_upgate, w_upval, w_down, out,
    buf_s, buf_a, buf_b, buf_c, buf_d, st_a, st_b, st_c, st_d,
    f_bgate, f_cgate, f_value, f_mixout, f_upgate, f_upval, f_down,
    xg, normed, gated, active, parts, zparts, recv_core, recv_x, recv_z,
    wz_send, wz_recv, wy_send, wy_recv, ag_z_send, ag_z_recv, ag_x_send, ag_x_recv,
    ag_c_send, ag_c_recv, rs_z_send, rs_z_recv, rs_zz_send, rs_zz_recv, rs_x_send, rs_x_recv, rs_c_send, rs_c_recv,
    local_sem,
):
    fs, me = lax.axis_index("fs"), lax.axis_index("tp")
    seqs, length, own = tok.shape
    width = own * n_tp
    planes, chips = n // 2, n_tp // 2
    bpo = n // n_tp
    bw = own // bpo
    sub = own // 2
    y, zz = fs % 2, fs // 2
    zi = zz % 2
    inner = (zz + zz // 2) % 2
    other = 1 - zi
    x, c = me // 2, me % 2
    blocks = f_upgate.shape[1] // 128
    full, odd = blocks // 2, blocks % 2
    second = full + odd
    down_rows = full * 128 + odd * 64

    def plane(r):
        result, bit = 0, 1
        while bit < planes:
            digit = zz // bit % 2
            result = result + bit * ((1 - digit) if r & bit else digit)
            bit *= 2
        return result

    def tp_of(r, core):
        return (x + r) % chips * 2 + core

    def remote(src, dst, send, recv, where):
        return pltpu.make_async_remote_copy(
            src_ref=src, dst_ref=dst, send_sem=send, recv_sem=recv,
            device_id=where, device_id_type=MESH,
        )

    bufs = (buf_s, buf_a, buf_a, buf_b, buf_c, buf_c, buf_d, buf_d)
    stages = (None, st_a, st_a, st_b, st_c, st_c, st_d, st_d)
    half = buf_c.shape[1] // 2
    low, high = pl.ds(0, half), pl.ds(half, half)
    spans = {A: low, F: high, C: low, E: high}
    spans[D] = pl.ds(0, down_rows // 2)
    spans[G] = pl.ds(down_rows // 2, down_rows // 2)

    def piece(g, at):
        return bufs[g].at[at, spans[g]] if g in spans else bufs[g].at[at]

    def stage(g):
        return stages[g].at[spans[g]] if g in spans else stages[g]

    def to_plane(g, r):
        src = stage(g) if r % 2 and g != S else piece(g, fs)
        return remote(
            src, piece(g, fs), wz_send.at[g, r - 1], wz_recv.at[g, r - 1],
            {"fs": plane(r) * 2 + y},
        )

    def to_row(g, r):
        at = piece(g, plane(r) * 2 + y)
        return remote(at, at, wy_send.at[g, r], wy_recv.at[g, r], {"fs": fs + 1 - 2 * y})

    def launch(g, rs):
        for r in rs:
            if r:
                to_plane(g, r).start()
            else:
                to_row(g, 0).start()

    def arrive(g, rs):
        for r in rs:
            to_plane(g, r).wait_recv()
            to_row(g, r).start()

    def complete(g):
        for r in range(planes):
            to_row(g, r).wait_recv()

    across = range(1, planes)
    rest = list(across)[:0:-1]

    def ag_z(k, s, src=None):
        at = xg.at[zi, me, s]
        return remote(
            at if src is None else src, at, ag_z_send.at[k, s], ag_z_recv.at[k, s],
            {"fs": fs + 2 - 4 * zi},
        )

    def ag_x(k, s, r, i, src=None):
        at = xg.at[other if i else zi, me, s]
        return remote(
            at if src is None else src, at, ag_x_send.at[k, s, r - 1, i],
            ag_x_recv.at[k, s, r - 1, i], {"tp": tp_of(r, c)},
        )

    def ag_c(k, s, r, i, src=None):
        at = xg.at[other if i else zi, tp_of(chips - r, c), s]
        return remote(
            at if src is None else src, at, ag_c_send.at[k, s, r, i], ag_c_recv.at[k, s, r, i],
            {"tp": me + 1 - 2 * c},
        )

    def gather_own(k, s, src=None):
        ag_z(k, s, src).start()
        for r in range(1, chips):
            ag_x(k, s, r, 0, src).start()
        ag_c(k, s, 0, 0, src).start()

    def gather_z(k, s):
        ag_z(k, s).wait_recv()
        for r in range(1, chips):
            ag_x(k, s, r, 1).start()
        ag_c(k, s, 0, 1).start()

    def gather_x(k, s):
        for i in (0, 1):
            for r in range(1, chips):
                ag_x(k, s, r, i).wait_recv()
                ag_c(k, s, r, i).start()

    def gather_done(k, s):
        for i in (0, 1):
            for r in range(chips):
                ag_c(k, s, r, i).wait_recv()

    def gather_sent(k):
        for s in range(seqs):
            if k == MIX:
                ag_z(k, s).wait_send()
            for i in (0, 1):
                for r in range(1, chips):
                    ag_x(k, s, r, i).wait_send()
                for r in range(chips):
                    ag_c(k, s, r, i).wait_send()

    def rs_c(k, s, r):
        return remote(
            parts.at[r, 1, s], recv_core.at[k, r, s], rs_c_send.at[k, s, r],
            rs_c_recv.at[k, s, r], {"tp": me + 1 - 2 * c},
        )

    def rs_x(k, s, r, j):
        i = zi if j else other
        return remote(
            parts.at[r, 0, s, i], recv_x.at[k, r - 1, s, i], rs_x_send.at[k, s, r - 1, j],
            rs_x_recv.at[k, s, r - 1, j], {"tp": tp_of(r, c)},
        )

    def rs_z(k, s, j):
        i = zi if j else other
        return remote(
            zparts.at[s, i], recv_z.at[k, s, i], rs_z_send.at[k, s, j], rs_z_recv.at[k, s, j],
            {"fs": fs + 2 - 4 * zi},
        )

    def products(k, s, r, side):
        owner = tp_of(r, 1 - c if side else c)
        source, held = ((gated, buf_b), (active, buf_d))[k]
        for b in range(bpo):
            at = owner * bpo + b
            lines = source[s].reshape(2 * length, source.shape[-1])
            part = jnp.dot(lines, held[at], preferred_element_type=F32)
            part = (part * buf_s[at, k : k + 1, :]).astype(BF16)
            parts[r, side, s, :, :, b * bw : (b + 1) * bw] = part.reshape(2, length, bw)

    order = list(range(1, chips)) + [0]
    tile = 64

    def scatter_begin(k, s, rs):
        for r in rs:
            products(k, s, r, 1)
            rs_c(k, s, r).start()
        for r in rs:
            products(k, s, r, 0)

    def away(r):
        return plane(r) // 2 != x

    def each_down(test, do, rs, groups=(D, G)):
        for r in rs:

            @pl.when(test(r))
            def _(r=r):
                for g in groups:
                    do(g, r)

    def down_across(rs):
        for r in rs:
            launch(D, [r])
            launch(G, [r])

    def down_arrive(first, rs, groups=(D, G)):
        each_down(lambda r: away(r) == first, lambda g, r: arrive(g, [r]), rs, groups)

    def down_complete(first):
        each_down(
            lambda r: away(r) == first, lambda g, r: to_row(g, r).wait_recv(), [0, 1] + rest
        )

    def scatter_x(k, s):
        for r in range(1, chips):
            rs_c(k, s, r).wait_recv()
            for part, i in enumerate((other, zi)):

                def step(j, carry, r=r, i=i):
                    at = pl.ds(pl.multiple_of(j * tile, tile), tile)
                    total = parts[r, 0, s, i, at, :].astype(F32)
                    total = total + recv_core[k, r, s, i, at, :].astype(F32)
                    parts[r, 0, s, i, at, :] = total.astype(BF16)
                    return carry

                lax.fori_loop(0, length // tile, step, 0)
                rs_x(k, s, r, part).start()

    def quad(k, s, i, at):
        total = parts[0, 0, s, i, at, :].astype(F32) + recv_core[k, 0, s, i, at, :].astype(F32)
        for r in range(1, chips):
            total = total + recv_x[k, r - 1, s, i, at, :].astype(F32)
        return total

    def scatter_z(k, s, j):
        i = zi if j else other
        if j == 0:
            rs_c(k, s, 0).wait_recv()
        for r in range(1, chips):
            rs_x(k, s, r, j).wait_recv()

        def step(line, carry):
            at = pl.ds(pl.multiple_of(line * tile, tile), tile)
            zparts[s, i, at, :] = quad(k, s, i, at).astype(BF16)
            return carry

        lax.fori_loop(0, length // tile, step, 0)
        rs_z(k, s, j).start()

    def resid(s, j):
        i = other if j else zi
        rs_z(MIX, s, j).wait_recv()

        def step(line, carry):
            at = pl.ds(pl.multiple_of(line * tile, tile), tile)
            total = zparts[s, i, at, :].astype(F32) + recv_z[MIX, s, i, at, :].astype(F32)
            xg[i, me, s, at, :] = (xg[i, me, s, at, :].astype(F32) + total).astype(BF16)
            return carry

        lax.fori_loop(0, length // tile, step, 0)
        for r in range(1, chips):
            ag_x(DOWN, s, r, j).start()
        ag_c(DOWN, s, 0, j).start()

    def rs_zz(s, r):
        return remote(
            zparts.at[s, r], recv_z.at[DOWN, s, r], rs_zz_send.at[s, r], rs_zz_recv.at[s, r],
            {"fs": fs + 2 - 4 * zi},
        )

    def rs_zx(s, r):
        return remote(
            parts.at[r, 0, s, zi], recv_x.at[DOWN, r - 1, s, 0], rs_x_send.at[DOWN, s, r - 1, 0],
            rs_x_recv.at[DOWN, s, r - 1, 0], {"tp": tp_of(r, c)},
        )

    def turned_z(s, rs):
        for r in rs:
            rs_c(DOWN, s, r).wait_recv()

            def step(j, carry, r=r):
                at = pl.ds(pl.multiple_of(j * tile, tile), tile)

                def pair(i):
                    total = parts[r, 0, s, i, at, :].astype(F32)
                    return total + recv_core[DOWN, r, s, i, at, :].astype(F32)

                zparts[s, r, at, :] = pair(other).astype(BF16)
                parts[r, 0, s, zi, at, :] = pair(zi).astype(BF16)
                return carry

            lax.fori_loop(0, length // tile, step, 0)
            rs_zz(s, r).start()

    def turned_x(s):
        for r in range(1, chips):
            rs_zz(s, r).wait_recv()

            def step(j, carry, r=r):
                at = pl.ds(pl.multiple_of(j * tile, tile), tile)
                total = parts[r, 0, s, zi, at, :].astype(F32)
                total = total + recv_z[DOWN, s, r, at, :].astype(F32)
                parts[r, 0, s, zi, at, :] = total.astype(BF16)
                return carry

            lax.fori_loop(0, length // tile, step, 0)
            rs_zx(s, r).start()

    def turned_finish(s):
        rs_zz(s, 0).wait_recv()
        for r in range(1, chips):
            rs_zx(s, r).wait_recv()

        def step(j, carry):
            at = pl.ds(pl.multiple_of(j * tile, tile), tile)
            total = parts[0, 0, s, zi, at, :].astype(F32)
            total = total + recv_z[DOWN, s, 0, at, :].astype(F32)
            for r in range(1, chips):
                total = total + recv_x[DOWN, r - 1, s, 0, at, :].astype(F32)
            out[s, at, :] = (xg[zi, me, s, at, :].astype(F32) + total).astype(BF16)
            return carry

        lax.fori_loop(0, length // tile, step, 0)

    def finish(s):
        rs_z(DOWN, s, 0).wait_recv()
        for r in range(1, chips):
            rs_x(DOWN, s, r, 1).wait_recv()

        def step(j, carry):
            at = pl.ds(pl.multiple_of(j * tile, tile), tile)
            total = quad(DOWN, s, zi, at) + recv_z[DOWN, s, zi, at, :].astype(F32)
            out[s, at, :] = (xg[zi, me, s, at, :].astype(F32) + total).astype(BF16)
            return carry

        lax.fori_loop(0, length // tile, step, 0)

    def scatter_sent(k):
        for s in range(seqs):
            turned = k == DOWN and s % 2
            for r in range(chips):
                rs_c(k, s, r).wait_send()
                if turned:
                    rs_zz(s, r).wait_send()
                if r and turned:
                    rs_zx(s, r).wait_send()
                elif r:
                    for j in (0, 1):
                        rs_x(k, s, r, j).wait_send()
            if not turned:
                for j in (0, 1) if k == MIX else (0,):
                    rs_z(k, s, j).wait_send()

    barrier = pltpu.get_barrier_semaphore()
    peers = [{"fs": plane(r) * 2 + y} for r in across]
    peers += [{"fs": fs + 1 - 2 * y}, {"tp": me + 1 - 2 * c}]
    peers += [{"tp": tp_of(r, c)} for r in range(1, chips)]
    for peer in peers:
        pl.semaphore_signal(barrier, inc=1, device_id=peer, device_id_type=MESH)

    sources = (w_bgate, w_cgate, w_value, w_mixout, w_upgate, w_upval, w_down)
    floats = (f_bgate, f_cgate, f_value, f_mixout, f_upgate, f_upval, f_down)
    loads = [
        pltpu.make_async_copy(source, held, local_sem.at[i])
        for i, (source, held) in enumerate(zip(sources, floats))
    ]
    for copy in loads:
        copy.start()

    def cast_rows(rows, put):
        step_rows = 32

        def step(i, carry):
            put(i * step_rows, step_rows)
            return carry

        lax.fori_loop(0, rows // step_rows, step, 0)

    def rows_at(start, count):
        return pl.ds(pl.multiple_of(start, 32), count)

    def lanes_at(start, count):
        return pl.ds(pl.multiple_of(start, 128), count)

    def put_in(start, count):
        at = rows_at(start, count)
        for i, held in enumerate((f_bgate, f_cgate, f_value)):
            cols = slice(i * sub, (i + 1) * sub)
            buf_a[fs, at, cols] = held[at, lanes_at(zi * sub, sub)].astype(BF16)
            st_a[at, cols] = held[at, lanes_at(other * sub, sub)].astype(BF16)

    def put_mixout(start, count):
        at = rows_at(start, count)
        buf_b[fs, at, :] = f_mixout[rows_at(zi * sub + start, count), :].astype(BF16)
        st_b[at, :] = f_mixout[rows_at(other * sub + start, count), :].astype(BF16)

    def put_up(start, count):
        at = rows_at(start, count)
        for j in range(full):
            for i, held in enumerate((f_upgate, f_upval)):
                cols = slice(j * 256 + i * 128, j * 256 + i * 128 + 128)
                mine = lanes_at((zi * second + j) * 128, 128)
                theirs = lanes_at((other * second + j) * 128, 128)
                buf_c[fs, at, cols] = held[at, mine].astype(BF16)
                st_c[at, cols] = held[at, theirs].astype(BF16)
        if odd:
            mid = slice(full * 128, full * 128 + 128)
            cols = slice(full * 256, full * 256 + 128)
            gate, val = f_upgate[at, mid], f_upval[at, mid]
            buf_c[fs, at, cols] = join_halves(gate, val, zi).astype(BF16)
            st_c[at, cols] = join_halves(gate, val, other).astype(BF16)

    def put_down(start, count):
        at = rows_at(start, count)
        buf_d[fs, at, :] = f_down[rows_at(zi * second * 128 + start, count), :].astype(BF16)
        st_d[at, :] = f_down[rows_at(other * second * 128 + start, count), :].astype(BF16)

    def put_down_mid(start, count):
        base = full * 128
        at = rows_at(base + start, count)
        buf_d[fs, at, :] = f_down[rows_at(base + zi * 64 + start, count), :].astype(BF16)
        st_d[at, :] = f_down[rows_at(base + other * 64 + start, count), :].astype(BF16)

    buf_s[fs] = jnp.zeros(buf_s.shape[1:], F32)
    buf_s[fs, 0:1, :] = mscale[...]
    buf_s[fs, 1:2, :] = dscale[...]
    for i in range(3):
        loads[i].wait()
    cast_rows(f_bgate.shape[0], put_in)
    pl.semaphore_wait(barrier, len(peers))

    launch(S, range(planes))
    gather_own(MIX, 0, tok.at[0])
    for g in (A, F):
        launch(g, [0, 1])
    for s in range(1, seqs):
        gather_own(MIX, s, tok.at[s])
    for r in rest:
        launch(A, [r])
        launch(F, [r])
    xg[zi, me] = tok[...]
    loads[3].wait()
    cast_rows(sub, put_mixout)
    launch(B, [0, 1])
    launch(B, rest)
    for i in (4, 5, 6):
        loads[i].wait()
    cast_rows(f_upgate.shape[0], put_up)
    cast_rows(full * 128, put_down)
    if odd:
        cast_rows(64, put_down_mid)
        for at in range(n):
            buf_d[at, down_rows:, :] = jnp.zeros((64, bw), BF16)

    def normalize(s, gain):
        step_rows = 32

        def step(j, carry):
            at = pl.ds(pl.multiple_of(j * step_rows, step_rows), step_rows)
            for i in (0, 1):
                squares = jnp.zeros((step_rows, 1), F32)
                for t in range(n_tp):
                    values = xg[i, t, s, at, :].astype(F32)
                    squares = squares + jnp.sum(values * values, axis=-1, keepdims=True)
                factor = lax.rsqrt(squares * (1.0 / width) + EPS)
                for t in range(n_tp):
                    cols = slice(t * own, (t + 1) * own)
                    values = xg[i, t, s, at, :].astype(F32)
                    normed[s, i, at, cols] = (values * factor * gain[:, cols]).astype(BF16)
            return carry

        lax.fori_loop(0, length // step_rows, step, 0)

    arrive(S, across)
    gather_z(MIX, 0)
    arrive(A, rest[:1])
    arrive(A, [1])
    gather_x(MIX, 0)
    arrive(F, rest[:1])
    arrive(F, [1])
    arrive(A, rest[1:])
    arrive(F, rest[1:])
    for s in range(1, seqs):
        gather_z(MIX, s)
    gather_done(MIX, 0)
    normalize(0, gain1)
    launch(C, [1])
    arrive(B, across)
    for s in range(1, seqs):
        gather_x(MIX, s)
        gather_done(MIX, s)
        normalize(s, gain1)
    launch(E, [1])
    for r in rest:
        launch(C, [r])
        launch(E, [r])
    launch(C, [0])
    complete(S)
    complete(A)
    complete(F)

    mixed = min(256, sub)

    def both_of(s):
        return normed[s].reshape(2 * length, width)

    def mixer(s):
        def step(j, carry):
            i, at = j % 2, j // 2 * mixed

            def product(m):
                cols = pl.ds(pl.multiple_of(m * sub + at, 128), mixed)
                matrix = buf_a[:, :, cols].reshape(width, mixed)
                return jnp.dot(normed[s, i], matrix, preferred_element_type=F32)

            here = pl.ds(pl.multiple_of(zi * sub + at, 128), mixed)
            scales = iscale[:, here]
            inner = (product(1) * scales[1:2]) * (product(2) * scales[2:3])
            convolved = causal_taps(inner, mtaps[:, here], 1)
            cols = pl.ds(pl.multiple_of(at, 128), mixed)
            gated[s, i, :, cols] = (product(0) * scales[0:1] * convolved).astype(BF16)
            return carry

        lax.fori_loop(0, 2 * (sub // mixed), step, 0)

    for s in range(seqs):
        mixer(s)
    gather_sent(MIX)
    arrive(C, [1])
    launch(E, [0])
    complete(B)
    for s in range(seqs):
        scatter_begin(MIX, s, order)
        scatter_x(MIX, s)
    arrive(E, [1])
    arrive(C, rest[:1])
    scatter_z(MIX, 0, 0)
    scatter_z(MIX, 0, 1)
    arrive(E, rest[:1])
    for s in range(1, seqs):
        scatter_z(MIX, s, 0)
        scatter_z(MIX, s, 1)
    resid(0, 0)
    arrive(C, rest[1:])
    resid(0, 1)
    pl.when((inner == 1) & away(0))(lambda: down_across(rest[:1]))
    arrive(E, rest[1:])
    down_across([0])
    gather_x(DOWN, 0)
    for s in range(1, seqs):
        resid(s, 0)
    pl.when(away(0))(lambda: down_across([1]))
    for s in range(1, seqs):
        resid(s, 1)
    pl.when((inner == 0) & away(0))(lambda: down_across(rest))
    gather_done(DOWN, 0)
    normalize(0, gain2)
    complete(C)
    complete(E)

    def up(s, first, last):
        def activate(gate, val):
            return gate / (1.0 + jnp.exp(-gate)) * val

        def step(t, carry):
            matrix = buf_c[:, :, lanes_at(t * 256, 256)].reshape(width, 256)
            both = jnp.dot(both_of(s), matrix, preferred_element_type=F32)
            here = lanes_at((zi * second + t) * 128, 128)
            gate = causal_taps(both[:, :128] * uscale[0:1, here], ftaps[:, 0, here], 2)
            val = causal_taps(both[:, 128:] * uscale[1:2, here], ftaps[:, 1, here], 2)
            values = activate(gate, val).astype(BF16)
            active[s, :, :, lanes_at(t * 128, 128)] = values.reshape(2, length, 128)
            return carry

        lax.fori_loop(first, last, step, 0)
        if odd and last == full:
            mid = slice(full * 128, full * 128 + 128)
            scale = join_halves(uscale[0:1, mid], uscale[1:2, mid], zi)
            taps = join_halves(ftaps[:, 0, mid], ftaps[:, 1, mid], zi)
            matrix = buf_c[:, :, full * 256 :].reshape(width, 128)
            both = jnp.dot(both_of(s), matrix, preferred_element_type=F32)
            gate = causal_taps(both * scale, taps, 2)
            values = activate(gate, pltpu.roll(gate, 64, 1))
            lanes = lax.broadcasted_iota(jnp.int32, values.shape, 1)
            values = jnp.where(lanes < 64, values, 0.0).astype(BF16)
            active[s, :, :, mid] = values.reshape(2, length, 128)

    up(0, 0, full // 2)
    pl.when((inner == 1) & away(0))(lambda: down_across(rest[1:]))
    up(0, full // 2, full)
    pl.when(jnp.logical_not(away(0)))(lambda: down_across([1] + rest))
    soon, late = [1] + rest[:1], rest[1:]
    for s in range(1, seqs):
        gather_x(DOWN, s)
    down_arrive(True, soon)
    for s in range(1, seqs):
        gather_done(DOWN, s)
        normalize(s, gain2)
        up(s, 0, full - full // 2)
    down_arrive(True, late, (D,))
    for s in range(1, seqs):
        up(s, full - full // 2, full)
    down_arrive(True, late, (G,))
    down_arrive(False, soon)
    scatter_sent(MIX)
    down_complete(True)
    far = order[:-1]
    for s in range(seqs):
        scatter_begin(DOWN, s, far)
        if s % 2:
            turned_z(s, far)
        else:
            scatter_x(DOWN, s)
    down_arrive(False, late)
    down_complete(False)
    for s in range(0, seqs, 2):
        scatter_begin(DOWN, s, [0])
        scatter_z(DOWN, s, 0)
    for s in range(1, seqs, 2):
        scatter_begin(DOWN, s, [0])
        turned_z(s, [0])
    for s in range(1, seqs, 2):
        turned_x(s)
    for s in range(seqs):
        if s % 2:
            turned_finish(s)
        else:
            finish(s)

    gather_sent(DOWN)
    scatter_sent(DOWN)
    for g in range(8):
        for r in range(planes):
            to_row(g, r).wait_send()
            if r:
                to_plane(g, r).wait_send()


def on_device(
    n,
    n_tp,
    tokens,
    mix_gain,
    w_bgate,
    w_cgate,
    w_value,
    in_scale,
    mix_taps,
    w_mixout,
    mixout_scale,
    ffn_gain,
    w_upgate,
    w_upval,
    up_scale,
    ffn_taps,
    w_down,
    down_scale,
):
    seqs, length, own = tokens.shape
    width = own * n_tp
    part = w_bgate.shape[0]
    ff = w_upgate.shape[1]
    pad = -ff % 128
    ffp = ff + pad
    bw = w_mixout.shape[1]

    if pad:
        w_upgate, w_upval, up_scale, ffn_taps = (
            jnp.pad(x, [(0, 0)] * (x.ndim - 1) + [(0, pad)])
            for x in (w_upgate, w_upval, up_scale, ffn_taps)
        )
        w_down = jnp.pad(w_down, ((0, pad), (0, 0)))
    weights = (w_bgate, w_cgate, w_value, w_mixout, w_upgate, w_upval, w_down)
    planes, chips, sub = n // 2, n_tp // 2, own // 2
    full, odd = ffp // 128 // 2, ffp // 128 % 2
    hidden, down_rows = (full + odd) * 128, full * 128 + odd * 64
    vmem, dma = pltpu.VMEM, pltpu.SemaphoreType.DMA
    result = pl.pallas_call(
        functools.partial(layer_kernel, n, n_tp),
        out_shape=jax.ShapeDtypeStruct((seqs, length, own), BF16),
        in_specs=[pl.BlockSpec(memory_space=pltpu.VMEM)] * 9
        + [pl.BlockSpec(memory_space=pl.ANY)] * 7,
        out_specs=pl.BlockSpec(memory_space=pltpu.VMEM),
        scratch_shapes=[
            vmem((n, 8, bw), F32),
            vmem((n, part, 3 * sub), BF16),
            vmem((n, sub, bw), BF16),
            vmem((n, part, ffp), BF16),
            vmem((n, hidden, bw), BF16),
            vmem((part, 3 * sub), BF16),
            vmem((sub, bw), BF16),
            vmem((part, ffp), BF16),
            vmem((down_rows, bw), BF16),
        ]
        + [vmem(w.shape, F32) for w in weights]
        + [
            vmem((2, n_tp, seqs, length, own), BF16),
            vmem((seqs, 2, length, width), BF16),
            vmem((seqs, 2, length, sub), BF16),
            vmem((seqs, 2, length, hidden), BF16),
            vmem((chips, 2, seqs, 2, length, own), BF16),
            vmem((seqs, max(2, chips), length, own), BF16),
            vmem((2, chips, seqs, 2, length, own), BF16),
            vmem((2, chips - 1, seqs, 2, length, own), BF16),
            vmem((2, seqs, max(2, chips), length, own), BF16),
            dma((8, planes - 1)),
            dma((8, planes - 1)),
            dma((8, planes)),
            dma((8, planes)),
            dma((2, seqs)),
            dma((2, seqs)),
            dma((2, seqs, chips - 1, 2)),
            dma((2, seqs, chips - 1, 2)),
            dma((2, seqs, chips, 2)),
            dma((2, seqs, chips, 2)),
            dma((2, seqs, 2)),
            dma((2, seqs, 2)),
            dma((seqs, chips)),
            dma((seqs, chips)),
            dma((2, seqs, chips - 1, 2)),
            dma((2, seqs, chips - 1, 2)),
            dma((2, seqs, chips)),
            dma((2, seqs, chips)),
            dma((7,)),
        ],
        compiler_params=pltpu.CompilerParams(
            collective_id=0, has_side_effects=True, vmem_limit_bytes=67043328
        ),
        name="layer",
    )(
        tokens, mix_gain.reshape(1, width), ffn_gain.reshape(1, width),
        in_scale, mix_taps, up_scale, ffn_taps.transpose(1, 0, 2), mixout_scale, down_scale, *weights,
    )
    return result


def solution(mesh):
    in_specs = (
        P("fs", None, "tp"),
        P(),
        P("fs", "tp"),
        P("fs", "tp"),
        P("fs", "tp"),
        P(None, "tp"),
        P(None, "tp"),
        P("tp", "fs"),
        P(None, "fs"),
        P(),
        P("fs", "tp"),
        P("fs", "tp"),
        P(None, "tp"),
        P(None, None, "tp"),
        P("tp", "fs"),
        P(None, "fs"),
    )
    out_specs = P("fs", None, "tp")
    body = functools.partial(on_device, mesh.shape["fs"], mesh.shape["tp"])
    return jax.shard_map(body, mesh=mesh, in_specs=in_specs, out_specs=out_specs, check_vma=False)
```

```python
import functools

import jax
import jax.numpy as jnp
from jax import lax
from jax.experimental import pallas as pl
from jax.experimental.pallas import tpu as pltpu
from jax.sharding import PartitionSpec as P

EPS = 1e-06
MESH = pl.DeviceIdType.MESH
F32 = jnp.float32
BF16 = jnp.bfloat16
S, A, F, B, C, E, D, G = range(8)
MIX, DOWN = 0, 1


def shifted(values, by, count):
    length = values.shape[0] // count
    rows = lax.broadcasted_iota(jnp.int32, values.shape, 0)
    keep = rows >= by
    for start in range(length, values.shape[0], length):
        keep &= (rows < start) | (rows >= start + by)
    return jnp.where(keep, pltpu.roll(values, by, 0), 0.0)


def causal_taps(values, taps, count):
    later = values * taps[2:3]
    return shifted(values, 2, count) * taps[0:1] + shifted(values, 1, count) * taps[1:2] + later


def join_halves(first, second, which):
    half = first.shape[-1] // 2
    lanes = lax.broadcasted_iota(jnp.int32, first.shape, 1)
    low = jnp.where(lanes < half, first, pltpu.roll(second, half, 1))
    high = jnp.where(lanes < half, pltpu.roll(first, half, 1), second)
    return jnp.where(which == 0, low, high)


def layer_kernel(
    n, n_tp, tok, gain1, gain2, iscale, mtaps, uscale, ftaps, mscale, dscale,
    w_bgate, w_cgate, w_value, w_mixout, w_upgate, w_upval, w_down, out,
    buf_s, buf_a, buf_b, buf_c, buf_d, st_a, st_b, st_c, st_d,
    f_bgate, f_cgate, f_value, f_mixout, f_upgate, f_upval, f_down,
    xg, normed, gated, active, parts, zparts, recv_core, recv_x, recv_z,
    wz_send, wz_recv, wy_send, wy_recv, ag_z_send, ag_z_recv, ag_x_send, ag_x_recv,
    ag_c_send, ag_c_recv, rs_z_send, rs_z_recv, rs_zz_send, rs_zz_recv, rs_x_send, rs_x_recv, rs_c_send, rs_c_recv,
    local_sem,
):
    fs, me = lax.axis_index("fs"), lax.axis_index("tp")
    seqs, length, own = tok.shape
    width = own * n_tp
    planes, chips = n // 2, n_tp // 2
    bpo = n // n_tp
    bw = own // bpo
    sub = own // 2
    y, zz = fs % 2, fs // 2
    zi = zz % 2
    inner = (zz + zz // 2) % 2
    other = 1 - zi
    x, c = me // 2, me % 2
    blocks = f_upgate.shape[1] // 128
    full, odd = blocks // 2, blocks % 2
    second = full + odd
    down_rows = full * 128 + odd * 64

    def plane(r):
        result, bit = 0, 1
        while bit < planes:
            digit = zz // bit % 2
            result = result + bit * ((1 - digit) if r & bit else digit)
            bit *= 2
        return result

    def tp_of(r, core):
        return (x + r) % chips * 2 + core

    def remote(src, dst, send, recv, where):
        return pltpu.make_async_remote_copy(
            src_ref=src, dst_ref=dst, send_sem=send, recv_sem=recv,
            device_id=where, device_id_type=MESH,
        )

    bufs = (buf_s, buf_a, buf_a, buf_b, buf_c, buf_c, buf_d, buf_d)
    stages = (None, st_a, st_a, st_b, st_c, st_c, st_d, st_d)
    half = buf_c.shape[1] // 2
    low, high = pl.ds(0, half), pl.ds(half, half)
    spans = {A: low, F: high, C: low, E: high}
    spans[D] = pl.ds(0, down_rows // 2)
    spans[G] = pl.ds(down_rows // 2, down_rows // 2)

    def piece(g, at):
        return bufs[g].at[at, spans[g]] if g in spans else bufs[g].at[at]

    def stage(g):
        return stages[g].at[spans[g]] if g in spans else stages[g]

    def to_plane(g, r):
        src = stage(g) if r % 2 and g != S else piece(g, fs)
        return remote(
            src, piece(g, fs), wz_send.at[g, r - 1], wz_recv.at[g, r - 1],
            {"fs": plane(r) * 2 + y},
        )

    def to_row(g, r):
        at = piece(g, plane(r) * 2 + y)
        return remote(at, at, wy_send.at[g, r], wy_recv.at[g, r], {"fs": fs + 1 - 2 * y})

    def launch(g, rs):
        for r in rs:
            if r:
                to_plane(g, r).start()
            else:
                to_row(g, 0).start()

    def arrive(g, rs):
        for r in rs:
            to_plane(g, r).wait_recv()
            to_row(g, r).start()

    def complete(g):
        for r in range(planes):
            to_row(g, r).wait_recv()

    across = range(1, planes)
    rest = list(across)[:0:-1]

    def ag_z(k, s, src=None):
        at = xg.at[zi, me, s]
        return remote(
            at if src is None else src, at, ag_z_send.at[k, s], ag_z_recv.at[k, s],
            {"fs": fs + 2 - 4 * zi},
        )

    def ag_x(k, s, r, i, src=None):
        at = xg.at[other if i else zi, me, s]
        return remote(
            at if src is None else src, at, ag_x_send.at[k, s, r - 1, i],
            ag_x_recv.at[k, s, r - 1, i], {"tp": tp_of(r, c)},
        )

    def ag_c(k, s, r, i, src=None):
        at = xg.at[other if i else zi, tp_of(chips - r, c), s]
        return remote(
            at if src is None else src, at, ag_c_send.at[k, s, r, i], ag_c_recv.at[k, s, r, i],
            {"tp": me + 1 - 2 * c},
        )

    def gather_own(k, s, src=None):
        ag_z(k, s, src).start()
        for r in range(1, chips):
            ag_x(k, s, r, 0, src).start()
        ag_c(k, s, 0, 0, src).start()

    def gather_z(k, s):
        ag_z(k, s).wait_recv()
        for r in range(1, chips):
            ag_x(k, s, r, 1).start()
        ag_c(k, s, 0, 1).start()

    def gather_x(k, s):
        for i in (0, 1):
            for r in range(1, chips):
                ag_x(k, s, r, i).wait_recv()
                ag_c(k, s, r, i).start()

    def gather_done(k, s):
        for i in (0, 1):
            for r in range(chips):
                ag_c(k, s, r, i).wait_recv()

    def gather_sent(k):
        for s in range(seqs):
            if k == MIX:
                ag_z(k, s).wait_send()
            for i in (0, 1):
                for r in range(1, chips):
                    ag_x(k, s, r, i).wait_send()
                for r in range(chips):
                    ag_c(k, s, r, i).wait_send()

    def rs_c(k, s, r):
        return remote(
            parts.at[r, 1, s], recv_core.at[k, r, s], rs_c_send.at[k, s, r],
            rs_c_recv.at[k, s, r], {"tp": me + 1 - 2 * c},
        )

    def rs_x(k, s, r, j):
        i = zi if j else other
        return remote(
            parts.at[r, 0, s, i], recv_x.at[k, r - 1, s, i], rs_x_send.at[k, s, r - 1, j],
            rs_x_recv.at[k, s, r - 1, j], {"tp": tp_of(r, c)},
        )

    def rs_z(k, s, j):
        i = zi if j else other
        return remote(
            zparts.at[s, i], recv_z.at[k, s, i], rs_z_send.at[k, s, j], rs_z_recv.at[k, s, j],
            {"fs": fs + 2 - 4 * zi},
        )

    def products(k, s, r, side):
        owner = tp_of(r, 1 - c if side else c)
        source, held = ((gated, buf_b), (active, buf_d))[k]
        for b in range(bpo):
            at = owner * bpo + b
            lines = source[s].reshape(2 * length, source.shape[-1])
            part = jnp.dot(lines, held[at], preferred_element_type=F32)
            part = (part * buf_s[at, k : k + 1, :]).astype(BF16)
            parts[r, side, s, :, :, b * bw : (b + 1) * bw] = part.reshape(2, length, bw)

    order = list(range(1, chips)) + [0]
    tile = 64

    def scatter_begin(k, s, rs):
        for r in rs:
            products(k, s, r, 1)
            rs_c(k, s, r).start()
        for r in rs:
            products(k, s, r, 0)

    def away(r):
        return plane(r) // 2 != x

    def each_down(test, do, rs, groups=(D, G)):
        for r in rs:

            @pl.when(test(r))
            def _(r=r):
                for g in groups:
                    do(g, r)

    def down_across(rs):
        for r in rs:
            launch(D, [r])
            launch(G, [r])

    def down_arrive(first, rs, groups=(D, G)):
        each_down(lambda r: away(r) == first, lambda g, r: arrive(g, [r]), rs, groups)

    def down_complete(first):
        each_down(
            lambda r: away(r) == first, lambda g, r: to_row(g, r).wait_recv(), [0, 1] + rest
        )

    def scatter_x(k, s):
        for r in range(1, chips):
            rs_c(k, s, r).wait_recv()
            for part, i in enumerate((other, zi)):

                def step(j, carry, r=r, i=i):
                    at = pl.ds(pl.multiple_of(j * tile, tile), tile)
                    total = parts[r, 0, s, i, at, :].astype(F32)
                    total = total + recv_core[k, r, s, i, at, :].astype(F32)
                    parts[r, 0, s, i, at, :] = total.astype(BF16)
                    return carry

                lax.fori_loop(0, length // tile, step, 0)
                rs_x(k, s, r, part).start()

    def quad(k, s, i, at):
        total = parts[0, 0, s, i, at, :].astype(F32) + recv_core[k, 0, s, i, at, :].astype(F32)
        for r in range(1, chips):
            total = total + recv_x[k, r - 1, s, i, at, :].astype(F32)
        return total

    def scatter_z(k, s, j):
        i = zi if j else other
        if j == 0:
            rs_c(k, s, 0).wait_recv()
        for r in range(1, chips):
            rs_x(k, s, r, j).wait_recv()

        def step(line, carry):
            at = pl.ds(pl.multiple_of(line * tile, tile), tile)
            zparts[s, i, at, :] = quad(k, s, i, at).astype(BF16)
            return carry

        lax.fori_loop(0, length // tile, step, 0)
        rs_z(k, s, j).start()

    def resid(s, j):
        i = other if j else zi
        rs_z(MIX, s, j).wait_recv()

        def step(line, carry):
            at = pl.ds(pl.multiple_of(line * tile, tile), tile)
            total = zparts[s, i, at, :].astype(F32) + recv_z[MIX, s, i, at, :].astype(F32)
            xg[i, me, s, at, :] = (xg[i, me, s, at, :].astype(F32) + total).astype(BF16)
            return carry

        lax.fori_loop(0, length // tile, step, 0)
        for r in range(1, chips):
            ag_x(DOWN, s, r, j).start()
        ag_c(DOWN, s, 0, j).start()

    def rs_zz(s, r):
        return remote(
            zparts.at[s, r], recv_z.at[DOWN, s, r], rs_zz_send.at[s, r], rs_zz_recv.at[s, r],
            {"fs": fs + 2 - 4 * zi},
        )

    def rs_zx(s, r):
        return remote(
            parts.at[r, 0, s, zi], recv_x.at[DOWN, r - 1, s, 0], rs_x_send.at[DOWN, s, r - 1, 0],
            rs_x_recv.at[DOWN, s, r - 1, 0], {"tp": tp_of(r, c)},
        )

    def turned_z(s, rs):
        for r in rs:
            rs_c(DOWN, s, r).wait_recv()

            def step(j, carry, r=r):
                at = pl.ds(pl.multiple_of(j * tile, tile), tile)

                def pair(i):
                    total = parts[r, 0, s, i, at, :].astype(F32)
                    return total + recv_core[DOWN, r, s, i, at, :].astype(F32)

                zparts[s, r, at, :] = pair(other).astype(BF16)
                parts[r, 0, s, zi, at, :] = pair(zi).astype(BF16)
                return carry

            lax.fori_loop(0, length // tile, step, 0)
            rs_zz(s, r).start()

    def turned_x(s):
        for r in range(1, chips):
            rs_zz(s, r).wait_recv()

            def step(j, carry, r=r):
                at = pl.ds(pl.multiple_of(j * tile, tile), tile)
                total = parts[r, 0, s, zi, at, :].astype(F32)
                total = total + recv_z[DOWN, s, r, at, :].astype(F32)
                parts[r, 0, s, zi, at, :] = total.astype(BF16)
                return carry

            lax.fori_loop(0, length // tile, step, 0)
            rs_zx(s, r).start()

    def turned_finish(s):
        rs_zz(s, 0).wait_recv()
        for r in range(1, chips):
            rs_zx(s, r).wait_recv()

        def step(j, carry):
            at = pl.ds(pl.multiple_of(j * tile, tile), tile)
            total = parts[0, 0, s, zi, at, :].astype(F32)
            total = total + recv_z[DOWN, s, 0, at, :].astype(F32)
            for r in range(1, chips):
                total = total + recv_x[DOWN, r - 1, s, 0, at, :].astype(F32)
            out[s, at, :] = (xg[zi, me, s, at, :].astype(F32) + total).astype(BF16)
            return carry

        lax.fori_loop(0, length // tile, step, 0)

    def finish(s):
        rs_z(DOWN, s, 0).wait_recv()
        for r in range(1, chips):
            rs_x(DOWN, s, r, 1).wait_recv()

        def step(j, carry):
            at = pl.ds(pl.multiple_of(j * tile, tile), tile)
            total = quad(DOWN, s, zi, at) + recv_z[DOWN, s, zi, at, :].astype(F32)
            out[s, at, :] = (xg[zi, me, s, at, :].astype(F32) + total).astype(BF16)
            return carry

        lax.fori_loop(0, length // tile, step, 0)

    def scatter_sent(k):
        for s in range(seqs):
            turned = k == DOWN and s % 2
            for r in range(chips):
                rs_c(k, s, r).wait_send()
                if turned:
                    rs_zz(s, r).wait_send()
                if r and turned:
                    rs_zx(s, r).wait_send()
                elif r:
                    for j in (0, 1):
                        rs_x(k, s, r, j).wait_send()
            if not turned:
                for j in (0, 1) if k == MIX else (0,):
                    rs_z(k, s, j).wait_send()

    barrier = pltpu.get_barrier_semaphore()
    peers = [{"fs": plane(r) * 2 + y} for r in across]
    peers += [{"fs": fs + 1 - 2 * y}, {"tp": me + 1 - 2 * c}]
    peers += [{"tp": tp_of(r, c)} for r in range(1, chips)]
    for peer in peers:
        pl.semaphore_signal(barrier, inc=1, device_id=peer, device_id_type=MESH)

    sources = (w_bgate, w_cgate, w_value, w_mixout, w_upgate, w_upval, w_down)
    floats = (f_bgate, f_cgate, f_value, f_mixout, f_upgate, f_upval, f_down)
    loads = [
        pltpu.make_async_copy(source, held, local_sem.at[i])
        for i, (source, held) in enumerate(zip(sources, floats))
    ]
    for copy in loads:
        copy.start()

    def cast_rows(rows, put):
        step_rows = 32

        def step(i, carry):
            put(i * step_rows, step_rows)
            return carry

        lax.fori_loop(0, rows // step_rows, step, 0)

    def rows_at(start, count):
        return pl.ds(pl.multiple_of(start, 32), count)

    def lanes_at(start, count):
        return pl.ds(pl.multiple_of(start, 128), count)

    def put_in(start, count):
        at = rows_at(start, count)
        for i, held in enumerate((f_bgate, f_cgate, f_value)):
            cols = slice(i * sub, (i + 1) * sub)
            buf_a[fs, at, cols] = held[at, lanes_at(zi * sub, sub)].astype(BF16)
            st_a[at, cols] = held[at, lanes_at(other * sub, sub)].astype(BF16)

    def put_mixout(start, count):
        at = rows_at(start, count)
        buf_b[fs, at, :] = f_mixout[rows_at(zi * sub + start, count), :].astype(BF16)
        st_b[at, :] = f_mixout[rows_at(other * sub + start, count), :].astype(BF16)

    def put_up(start, count):
        at = rows_at(start, count)
        for j in range(full):
            for i, held in enumerate((f_upgate, f_upval)):
                cols = slice(j * 256 + i * 128, j * 256 + i * 128 + 128)
                mine = lanes_at((zi * second + j) * 128, 128)
                theirs = lanes_at((other * second + j) * 128, 128)
                buf_c[fs, at, cols] = held[at, mine].astype(BF16)
                st_c[at, cols] = held[at, theirs].astype(BF16)
        if odd:
            mid = slice(full * 128, full * 128 + 128)
            cols = slice(full * 256, full * 256 + 128)
            gate, val = f_upgate[at, mid], f_upval[at, mid]
            buf_c[fs, at, cols] = join_halves(gate, val, zi).astype(BF16)
            st_c[at, cols] = join_halves(gate, val, other).astype(BF16)

    def put_down(start, count):
        at = rows_at(start, count)
        buf_d[fs, at, :] = f_down[rows_at(zi * second * 128 + start, count), :].astype(BF16)
        st_d[at, :] = f_down[rows_at(other * second * 128 + start, count), :].astype(BF16)

    def put_down_mid(start, count):
        base = full * 128
        at = rows_at(base + start, count)
        buf_d[fs, at, :] = f_down[rows_at(base + zi * 64 + start, count), :].astype(BF16)
        st_d[at, :] = f_down[rows_at(base + other * 64 + start, count), :].astype(BF16)

    buf_s[fs] = jnp.zeros(buf_s.shape[1:], F32)
    buf_s[fs, 0:1, :] = mscale[...]
    buf_s[fs, 1:2, :] = dscale[...]
    for i in range(3):
        loads[i].wait()
    cast_rows(f_bgate.shape[0], put_in)
    pl.semaphore_wait(barrier, len(peers))

    launch(S, range(planes))
    gather_own(MIX, 0, tok.at[0])
    for g in (A, F):
        launch(g, [0, 1])
    for s in range(1, seqs):
        gather_own(MIX, s, tok.at[s])
    for r in rest:
        launch(A, [r])
        launch(F, [r])
    xg[zi, me] = tok[...]
    loads[3].wait()
    cast_rows(sub, put_mixout)
    launch(B, [0, 1])
    launch(B, rest)
    for i in (4, 5, 6):
        loads[i].wait()
    cast_rows(f_upgate.shape[0], put_up)
    cast_rows(full * 128, put_down)
    if odd:
        cast_rows(64, put_down_mid)
        for at in range(n):
            buf_d[at, down_rows:, :] = jnp.zeros((64, bw), BF16)

    def normalize(s, gain):
        step_rows = 32

        def step(j, carry):
            at = pl.ds(pl.multiple_of(j * step_rows, step_rows), step_rows)
            for i in (0, 1):
                squares = jnp.zeros((step_rows, 1), F32)
                for t in range(n_tp):
                    values = xg[i, t, s, at, :].astype(F32)
                    squares = squares + jnp.sum(values * values, axis=-1, keepdims=True)
                factor = lax.rsqrt(squares * (1.0 / width) + EPS)
                for t in range(n_tp):
                    cols = slice(t * own, (t + 1) * own)
                    values = xg[i, t, s, at, :].astype(F32)
                    normed[s, i, at, cols] = (values * factor * gain[:, cols]).astype(BF16)
            return carry

        lax.fori_loop(0, length // step_rows, step, 0)

    arrive(S, across)
    gather_z(MIX, 0)
    arrive(A, rest[:1])
    arrive(A, [1])
    gather_x(MIX, 0)
    arrive(F, rest[:1])
    arrive(F, [1])
    arrive(A, rest[1:])
    arrive(F, rest[1:])
    for s in range(1, seqs):
        gather_z(MIX, s)
    gather_done(MIX, 0)
    normalize(0, gain1)
    launch(C, [1])
    arrive(B, across)
    for s in range(1, seqs):
        gather_x(MIX, s)
        gather_done(MIX, s)
        normalize(s, gain1)
    launch(E, [1])
    for r in rest:
        launch(C, [r])
        launch(E, [r])
    launch(C, [0])
    complete(S)
    complete(A)
    complete(F)

    mixed = min(256, sub)

    def both_of(s):
        return normed[s].reshape(2 * length, width)

    def mixer(s):
        def step(j, carry):
            i, at = j % 2, j // 2 * mixed

            def product(m):
                cols = pl.ds(pl.multiple_of(m * sub + at, 128), mixed)
                matrix = buf_a[:, :, cols].reshape(width, mixed)
                return jnp.dot(normed[s, i], matrix, preferred_element_type=F32)

            here = pl.ds(pl.multiple_of(zi * sub + at, 128), mixed)
            scales = iscale[:, here]
            inner = (product(1) * scales[1:2]) * (product(2) * scales[2:3])
            convolved = causal_taps(inner, mtaps[:, here], 1)
            cols = pl.ds(pl.multiple_of(at, 128), mixed)
            gated[s, i, :, cols] = (product(0) * scales[0:1] * convolved).astype(BF16)
            return carry

        lax.fori_loop(0, 2 * (sub // mixed), step, 0)

    for s in range(seqs):
        mixer(s)
    gather_sent(MIX)
    arrive(C, [1])
    launch(E, [0])
    complete(B)
    for s in range(seqs):
        scatter_begin(MIX, s, order)
        scatter_x(MIX, s)
    arrive(E, [1])
    arrive(C, rest[:1])
    scatter_z(MIX, 0, 0)
    scatter_z(MIX, 0, 1)
    pl.when(inner == 0)(lambda: arrive(E, rest[:1]))
    for s in range(1, seqs):
        scatter_z(MIX, s, 0)
        scatter_z(MIX, s, 1)
    pl.when(inner == 1)(lambda: arrive(E, rest[:1]))
    resid(0, 0)
    arrive(C, rest[1:])
    resid(0, 1)
    pl.when((inner == 1) & away(0))(lambda: down_across(rest[:1]))
    arrive(E, rest[1:])
    down_across([0])
    gather_x(DOWN, 0)
    for s in range(1, seqs):
        resid(s, 0)
    pl.when(away(0))(lambda: down_across([1]))
    for s in range(1, seqs):
        resid(s, 1)
    pl.when((inner == 0) & away(0))(lambda: down_across(rest))
    gather_done(DOWN, 0)
    normalize(0, gain2)
    complete(C)
    complete(E)

    def up(s, first, last):
        def activate(gate, val):
            return gate / (1.0 + jnp.exp(-gate)) * val

        def step(t, carry):
            matrix = buf_c[:, :, lanes_at(t * 256, 256)].reshape(width, 256)
            both = jnp.dot(both_of(s), matrix, preferred_element_type=F32)
            here = lanes_at((zi * second + t) * 128, 128)
            gate = causal_taps(both[:, :128] * uscale[0:1, here], ftaps[:, 0, here], 2)
            val = causal_taps(both[:, 128:] * uscale[1:2, here], ftaps[:, 1, here], 2)
            values = activate(gate, val).astype(BF16)
            active[s, :, :, lanes_at(t * 128, 128)] = values.reshape(2, length, 128)
            return carry

        lax.fori_loop(first, last, step, 0)
        if odd and last == full:
            mid = slice(full * 128, full * 128 + 128)
            scale = join_halves(uscale[0:1, mid], uscale[1:2, mid], zi)
            taps = join_halves(ftaps[:, 0, mid], ftaps[:, 1, mid], zi)
            matrix = buf_c[:, :, full * 256 :].reshape(width, 128)
            both = jnp.dot(both_of(s), matrix, preferred_element_type=F32)
            gate = causal_taps(both * scale, taps, 2)
            values = activate(gate, pltpu.roll(gate, 64, 1))
            lanes = lax.broadcasted_iota(jnp.int32, values.shape, 1)
            values = jnp.where(lanes < 64, values, 0.0).astype(BF16)
            active[s, :, :, mid] = values.reshape(2, length, 128)

    pl.when((inner == 1) & away(0))(lambda: down_across(rest[1:]))
    up(0, 0, full)
    pl.when(jnp.logical_not(away(0)))(lambda: down_across([1] + rest))
    soon, late = [1] + rest[:1], rest[1:]
    for s in range(1, seqs):
        gather_x(DOWN, s)
    down_arrive(True, soon)
    for s in range(1, seqs):
        gather_done(DOWN, s)
        normalize(s, gain2)
        up(s, 0, full - full // 2)
    down_arrive(True, late, (D,))
    for s in range(1, seqs):
        up(s, full - full // 2, full)
    down_arrive(True, late, (G,))
    down_arrive(False, soon)
    scatter_sent(MIX)
    down_complete(True)
    far = order[:-1]
    for s in range(seqs):
        scatter_begin(DOWN, s, far)
    for s in range(seqs):
        if s % 2:
            turned_z(s, far)
        else:
            scatter_x(DOWN, s)
    down_arrive(False, late)
    down_complete(False)
    for s in range(0, seqs, 2):
        scatter_begin(DOWN, s, [0])
        scatter_z(DOWN, s, 0)
    for s in range(1, seqs, 2):
        scatter_begin(DOWN, s, [0])
        turned_z(s, [0])
    for s in range(1, seqs, 2):
        turned_x(s)
    for s in range(seqs):
        if s % 2:
            turned_finish(s)
        else:
            finish(s)

    gather_sent(DOWN)
    scatter_sent(DOWN)
    for g in range(8):
        for r in range(planes):
            to_row(g, r).wait_send()
            if r:
                to_plane(g, r).wait_send()


def on_device(
    n,
    n_tp,
    tokens,
    mix_gain,
    w_bgate,
    w_cgate,
    w_value,
    in_scale,
    mix_taps,
    w_mixout,
    mixout_scale,
    ffn_gain,
    w_upgate,
    w_upval,
    up_scale,
    ffn_taps,
    w_down,
    down_scale,
):
    seqs, length, own = tokens.shape
    width = own * n_tp
    part = w_bgate.shape[0]
    ff = w_upgate.shape[1]
    pad = -ff % 128
    ffp = ff + pad
    bw = w_mixout.shape[1]

    if pad:
        w_upgate, w_upval, up_scale, ffn_taps = (
            jnp.pad(x, [(0, 0)] * (x.ndim - 1) + [(0, pad)])
            for x in (w_upgate, w_upval, up_scale, ffn_taps)
        )
        w_down = jnp.pad(w_down, ((0, pad), (0, 0)))
    weights = (w_bgate, w_cgate, w_value, w_mixout, w_upgate, w_upval, w_down)
    planes, chips, sub = n // 2, n_tp // 2, own // 2
    full, odd = ffp // 128 // 2, ffp // 128 % 2
    hidden, down_rows = (full + odd) * 128, full * 128 + odd * 64
    vmem, dma = pltpu.VMEM, pltpu.SemaphoreType.DMA
    result = pl.pallas_call(
        functools.partial(layer_kernel, n, n_tp),
        out_shape=jax.ShapeDtypeStruct((seqs, length, own), BF16),
        in_specs=[pl.BlockSpec(memory_space=pltpu.VMEM)] * 9
        + [pl.BlockSpec(memory_space=pl.ANY)] * 7,
        out_specs=pl.BlockSpec(memory_space=pltpu.VMEM),
        scratch_shapes=[
            vmem((n, 8, bw), F32),
            vmem((n, part, 3 * sub), BF16),
            vmem((n, sub, bw), BF16),
            vmem((n, part, ffp), BF16),
            vmem((n, hidden, bw), BF16),
            vmem((part, 3 * sub), BF16),
            vmem((sub, bw), BF16),
            vmem((part, ffp), BF16),
            vmem((down_rows, bw), BF16),
        ]
        + [vmem(w.shape, F32) for w in weights]
        + [
            vmem((2, n_tp, seqs, length, own), BF16),
            vmem((seqs, 2, length, width), BF16),
            vmem((seqs, 2, length, sub), BF16),
            vmem((seqs, 2, length, hidden), BF16),
            vmem((chips, 2, seqs, 2, length, own), BF16),
            vmem((seqs, max(2, chips), length, own), BF16),
            vmem((2, chips, seqs, 2, length, own), BF16),
            vmem((2, chips - 1, seqs, 2, length, own), BF16),
            vmem((2, seqs, max(2, chips), length, own), BF16),
            dma((8, planes - 1)),
            dma((8, planes - 1)),
            dma((8, planes)),
            dma((8, planes)),
            dma((2, seqs)),
            dma((2, seqs)),
            dma((2, seqs, chips - 1, 2)),
            dma((2, seqs, chips - 1, 2)),
            dma((2, seqs, chips, 2)),
            dma((2, seqs, chips, 2)),
            dma((2, seqs, 2)),
            dma((2, seqs, 2)),
            dma((seqs, chips)),
            dma((seqs, chips)),
            dma((2, seqs, chips - 1, 2)),
            dma((2, seqs, chips - 1, 2)),
            dma((2, seqs, chips)),
            dma((2, seqs, chips)),
            dma((7,)),
        ],
        compiler_params=pltpu.CompilerParams(
            collective_id=0, has_side_effects=True, vmem_limit_bytes=67043328
        ),
        name="layer",
    )(
        tokens, mix_gain.reshape(1, width), ffn_gain.reshape(1, width),
        in_scale, mix_taps, up_scale, ffn_taps.transpose(1, 0, 2), mixout_scale, down_scale, *weights,
    )
    return result


def solution(mesh):
    in_specs = (
        P("fs", None, "tp"),
        P(),
        P("fs", "tp"),
        P("fs", "tp"),
        P("fs", "tp"),
        P(None, "tp"),
        P(None, "tp"),
        P("tp", "fs"),
        P(None, "fs"),
        P(),
        P("fs", "tp"),
        P("fs", "tp"),
        P(None, "tp"),
        P(None, None, "tp"),
        P("tp", "fs"),
        P(None, "fs"),
    )
    out_specs = P("fs", None, "tp")
    body = functools.partial(on_device, mesh.shape["fs"], mesh.shape["tp"])
    return jax.shard_map(body, mesh=mesh, in_specs=in_specs, out_specs=out_specs, check_vma=False)
```
